32 devices in a mesh: kv: 8 (over z, x), tp: 4 (over y, core).
Axes of the slice: x: 2, y: 2, z: 4, core: 2. Of those that a mesh axis runs over, the one named last changes fastest.
Arguments:
- activations: bfloat16 [384, 2048], P(None, ('kv', 'tp')), may hold values from -6 to 6
- latent_cache: bfloat16 [24, 16384, 288], P(None, 'kv'), may hold values from -6 to 6
- lengths: int32 [24], replicated, may hold values from 4096 to 16352, as said below
- accepted: int32 [24], replicated, may hold values from 0 to 16
- parents: int32 [24, 16], replicated, may hold values from -1 to 14, as said below
- w_query_down: bfloat16 [2048, 512], P(('kv', 'tp')), may hold values from -0.125 to 0.125
- w_key_down: bfloat16 [2048, 288], P(('kv', 'tp')), may hold values from -0.125 to 0.125
- gain_input: bfloat16 [2048], P(('kv', 'tp')), may hold values from 0.099609375 to 1.8984375
- gain_query: bfloat16 [512], replicated, may hold values from 0.099609375 to 1.8984375
- gain_key: bfloat16 [256], replicated, may hold values from 0.099609375 to 1.8984375
- w_query: bfloat16 [512, 16, 288], P(None, 'tp'), as said below
- w_value: bfloat16 [16, 256, 64], replicated, may hold values from -0.375 to 0.375
- w_out: bfloat16 [1024, 2048], P('tp', 'kv'), may hold values from -1 to 1, as said below
- gain_output: bfloat16 [2048], P('kv'), may hold values from 0.099609375 to 1.8984375
Outputs:
- mixed: bfloat16 [384, 2048], P(None, 'kv')
- new_cache: bfloat16 [24, 16384, 288], P(None, 'kv')
The draws below stay inside these ranges and needn't reach their ends.
Inputs may be any that keep to these rules, and one draw needn't show every extreme that they name: One sequence has lengths exactly 16352 and another exactly 4096; which ones varies. accepted is between 0 and 16, so the proposals' positions lie below 16384. `parents`: the parent of proposal i is -1 or a proposal with a smaller index; proposal 0 has parent -1; the proposals of exactly one sequence (which one varies) form a single chain; the other sequences' proposals form general trees. `w_query`: entries are normal with standard deviation (1536)^(-1/2) cut at six standard deviations; in the hidden draw the heads whose index is a multiple of 4 are 48 times larger. `w_out`: entries of order (1024)^(-1/2).
All inputs are finite; a program needn't handle non-finite values.
Results may differ from the reference program's by a relative error of at most 0.0096.
The reference program's roundings to bfloat16 on the way count: a program that leaves them out, or rounds other values in their place, can miss the bound.
Values may be sent and summed in bfloat16 or wider, within the bound.
A program may use at most 192 MiB of HBM per device.

```python
import jax
import jax.numpy as jnp
from jax import lax

D = 2048
HEADS = 16
Q_RANK = 512
KV_RANK = 256
ROPE_DIM = 32
NOPE_DIM = 64
V_DIM = 64
PROPS = 16
SEQS = 24
POS_DEV = 2048
CACHE_LEN = 16384
ROWS = 384
N_KV = 8


def draw_w_query(key, part):
    spread = (3.0 * Q_RANK) ** (-0.5)
    drawn = jnp.clip(jax.random.normal(key, (Q_RANK, HEADS, KV_RANK + ROPE_DIM), jnp.float32), -6.0, 6.0) * spread
    return drawn.astype(jnp.bfloat16)


def draw_w_out(key, part):
    fan_width = HEADS * V_DIM
    spread = float(fan_width) ** (-0.5)
    base_key = jax.random.fold_in(key, 31)
    left_key = jax.random.fold_in(key, 32)
    right_key = jax.random.fold_in(key, 33)
    turn_key = jax.random.fold_in(key, 34)
    base = jnp.clip(jax.random.normal(base_key, (fan_width, D), jnp.float32), -4.0, 4.0) * spread
    left_signs = jnp.where(jax.random.bernoulli(left_key, 0.5, (fan_width,)), 1.0, -1.0).astype(jnp.float32)
    right_signs = jnp.where(jax.random.bernoulli(right_key, 0.5, (D,)), 1.0, -1.0).astype(jnp.float32)
    drawn = base + spread * left_signs[:, None] * right_signs[None, :]
    heading = jnp.where(jax.random.bernoulli(turn_key, 0.5, ()), 1.0, -1.0).astype(jnp.float32)
    column_pos = jnp.arange(D, dtype=jnp.float32) / float(D - 1) - 0.5
    column_scale = jnp.exp(heading * column_pos * jnp.log(3.0))
    drawn = drawn * column_scale[None, :]
    return drawn.astype(jnp.bfloat16)


def draw_lengths(key, part):
    value_key = jax.random.fold_in(key, 11)
    pick_key = jax.random.fold_in(key, 12)
    step_key = jax.random.fold_in(key, 13)
    drawn = jax.random.randint(value_key, (SEQS,), CACHE_LEN // 4, CACHE_LEN - 2 * PROPS + 1)
    seq_ids = jnp.arange(SEQS, dtype=jnp.int32)
    longest = jax.random.randint(pick_key, (), 0, SEQS)
    shortest = (longest + jax.random.randint(step_key, (), 1, SEQS)) % SEQS
    drawn = jnp.where(seq_ids == shortest, CACHE_LEN // 4, drawn)
    drawn = jnp.where(seq_ids == longest, CACHE_LEN - 2 * PROPS, drawn)
    return drawn.astype(jnp.int32)


def draw_parents(key, part):
    link_key = jax.random.fold_in(key, 21)
    pick_key = jax.random.fold_in(key, 22)
    slot_ids = jnp.arange(PROPS, dtype=jnp.int32)
    drawn = jax.random.randint(link_key, (SEQS, PROPS), -1, slot_ids[None, :])
    drawn = jnp.where(slot_ids[None, :] == 0, -1, drawn)
    chain_links = slot_ids - 1
    chained = jax.random.randint(pick_key, (), 0, SEQS)
    chain_seq = (jnp.arange(SEQS, dtype=jnp.int32) == chained)[:, None]
    return jnp.where(chain_seq, chain_links[None, :], drawn).astype(jnp.int32)


def set_ends(result, own_key, least, high):
    place = [jax.random.randint(jax.random.fold_in(own_key, axis), (), 0, length) for axis, length in enumerate(result.shape)]
    main_axis = result.shape.index(max(result.shape))
    neighbour = place[:main_axis] + [(place[main_axis] + 1) % result.shape[main_axis]] + place[main_axis + 1:]
    return result.at[tuple(place)].set(least).at[tuple(neighbour)].set(high)


def levels(own_key, shape, shards, smallest, top_value):
    def one(position, parts):
        draws = jax.random.uniform(jax.random.fold_in(jax.random.fold_in(own_key, 6), position), (parts,), jnp.float32, smallest / len(shards), top_value / len(shards))
        return jnp.repeat(jnp.exp(draws), shape[position] // parts).reshape((-1,) + (1,) * (len(shape) - position - 1))

    level = one(*shards[0])
    for cut in shards[1:]:
        level = level * one(*cut)
    return level


def bell_draw(own_key, shape, deviation, reach, pieces=(), held_as=jnp.bfloat16):
    values = jax.random.normal(own_key, shape, jnp.float32) * deviation
    if len(pieces) > 0:
        values = levels(own_key, shape, pieces, -0.22, 0.18) * values
    return jnp.clip(values, min=-reach, max=reach).astype(held_as)


def setup_inputs(seed: int = 0) -> dict:
    key_of = jax.random.split(jax.random.key(seed), 15)
    activations = bell_draw(key_of[0], (ROWS, D), 1.0, 6.0, ((1, 32),))
    latent_cache = bell_draw(key_of[1], (SEQS, CACHE_LEN, KV_RANK + ROPE_DIM), 1.0, 6.0, ((1, 8),))
    lengths = draw_lengths(jax.random.fold_in(key_of[14], 71), 0)
    accepted = set_ends(jax.random.randint(key_of[3], (SEQS,), 0, PROPS + 1), jax.random.fold_in(key_of[3], 1), 0, PROPS).astype(jnp.int32)
    parents = draw_parents(jax.random.fold_in(key_of[14], 71), 0)
    w_query_down = bell_draw(key_of[5], (D, Q_RANK), D ** -0.5, 0.125, ((0, 32),))
    w_key_down = bell_draw(key_of[6], (D, KV_RANK + ROPE_DIM), D ** -0.5, 0.125, ((0, 32),))
    gain_input = jnp.clip(1.0 + 0.18 * jax.random.normal(key_of[7], (D,), jnp.float32), 0.099609375, 1.8984375).astype(jnp.bfloat16)
    gain_query = jnp.clip(1.0 + 0.18 * jax.random.normal(key_of[8], (Q_RANK,), jnp.float32), 0.099609375, 1.8984375).astype(jnp.bfloat16)
    gain_key = jnp.clip(1.0 + 0.18 * jax.random.normal(key_of[9], (KV_RANK,), jnp.float32), 0.099609375, 1.8984375).astype(jnp.bfloat16)
    w_query = draw_w_query(jax.random.fold_in(key_of[14], 71), 0)
    w_value = bell_draw(key_of[11], (HEADS, KV_RANK, V_DIM), KV_RANK ** -0.5, 0.375)
    w_out = draw_w_out(jax.random.fold_in(key_of[14], 71), 0)
    gain_output = jnp.clip(1.0 + 0.18 * jax.random.normal(key_of[13], (D,), jnp.float32), 0.099609375, 1.8984375).astype(jnp.bfloat16)
    return {"activations": activations, "latent_cache": latent_cache, "lengths": lengths, "accepted": accepted, "parents": parents, "w_query_down": w_query_down, "w_key_down": w_key_down, "gain_input": gain_input, "gain_query": gain_query, "gain_key": gain_key, "w_query": w_query, "w_value": w_value, "w_out": w_out, "gain_output": gain_output}


epsilon = 1e-06
rope_base = 10000.0
score_after_mask = -1e+30

def rotate(component, places):
    half_width = component.shape[-1] // 2
    frequency = rope_base ** (-jnp.arange(half_width, dtype=jnp.float32) / half_width)
    angles = places.astype(jnp.float32)[:, None] * frequency[None, :]
    target_shape = (places.shape[0],) + (1,) * (component.ndim - 2) + (half_width,)
    cosine = jnp.cos(angles).reshape(target_shape)
    sine_part = jnp.sin(angles).reshape(target_shape)
    front_half = component[..., :half_width]
    back_half = component[..., half_width:]
    return jnp.concatenate([front_half * cosine - back_half * sine_part, back_half * cosine + front_half * sine_part], axis=-1)

def normalize(values, scales):
    return values * lax.rsqrt(lax.optimization_barrier(jnp.mean(values * values, axis=-1, keepdims=True)) + epsilon) * scales.astype(jnp.float32)

def ancestry(parents):
    seq_count, prop_count = parents.shape
    slot_ids = jnp.arange(prop_count, dtype=jnp.int32)
    parent_links = (parents[:, :, None] == slot_ids[None, None, :]).astype(jnp.float32)
    identity = jnp.broadcast_to(jnp.eye(prop_count, dtype=jnp.float32), parent_links.shape)
    reached = jnp.minimum(identity + parent_links, 1.0)
    for repeat in range((prop_count - 1).bit_length()):
        reached = jnp.minimum(jnp.einsum('sij,sjk->sik', reached, reached, precision=lax.Precision.HIGHEST), 1.0)
    depths = (lax.optimization_barrier(jnp.sum(reached, axis=-1)) - 1.0).astype(jnp.int32)
    return (reached, depths)

def partial_attend(queries, key_rows, slot_index, onehot, reached, w_value):
    score_scale = (NOPE_DIM + ROPE_DIM) ** (-0.5)
    ancestors = jnp.einsum('sij,snj->sin', reached, onehot, precision=lax.Precision.HIGHEST)
    visible = ((slot_index < 0)[:, None, :] | (ancestors > 0.5))[:, :, None, :]
    scores = jnp.einsum('siha,sna->sihn', queries.astype(jnp.float32), key_rows.astype(jnp.float32), precision=lax.Precision.HIGHEST) * score_scale
    masked = jnp.where(visible, scores, score_after_mask)
    maxima = lax.optimization_barrier(jnp.max(masked, axis=-1))
    weights = jnp.where(visible, jnp.exp(masked - maxima[..., None]), 0.0)
    totals = lax.optimization_barrier(jnp.sum(weights, axis=-1))
    rounded = lax.optimization_barrier(weights.astype(jnp.bfloat16))
    weighted = jnp.einsum('sihn,snk->sihk', rounded.astype(jnp.float32), key_rows[:, :, :KV_RANK].astype(jnp.float32), precision=lax.Precision.HIGHEST)
    value_fraction = lax.optimization_barrier((weighted / jnp.maximum(totals, 1.0)[..., None]).astype(jnp.bfloat16))
    values = jnp.einsum('siha,hav->sihv', value_fraction.astype(jnp.float32), w_value.astype(jnp.float32), precision=lax.Precision.HIGHEST).astype(jnp.bfloat16)
    return (maxima, totals, values)

def combine_parts(maxima, totals, values):
    largest = lax.optimization_barrier(jnp.max(maxima, axis=0))
    shares = totals * jnp.exp(maxima - largest[None])
    summed = lax.optimization_barrier(jnp.sum(shares[..., None] * values.astype(jnp.float32), axis=0))
    return summed / lax.optimization_barrier(jnp.sum(shares, axis=0))[..., None]

def location_rows(seq_cache, rows_of, anchor):
    return lax.dynamic_update_slice(seq_cache, rows_of, (anchor, jnp.int32(0)))

def reference(activations, latent_cache, lengths, accepted, parents, w_query_down, w_key_down, gain_input, gain_query, gain_key, w_query, w_value, w_out, gain_output):
    reached, depths = ancestry(parents)
    filled = lengths + accepted
    places = (filled[:, None] + depths).reshape(-1)
    as_float = activations.astype(jnp.float32)
    scaled = (as_float * gain_input.astype(jnp.float32)).astype(jnp.bfloat16)
    inverse = lax.rsqrt(lax.optimization_barrier(jnp.mean(as_float * as_float, axis=-1, keepdims=True)) + epsilon)
    query_raw = jnp.dot(scaled, w_query_down, preferred_element_type=jnp.float32) * inverse
    key_raw = jnp.dot(scaled, w_key_down, preferred_element_type=jnp.float32) * inverse
    query_low = normalize(query_raw, gain_query).astype(jnp.bfloat16)
    mapped_output = jnp.dot(query_low, w_query.reshape(Q_RANK, -1), preferred_element_type=jnp.float32)
    mapped_output = mapped_output.reshape(ROWS, HEADS, KV_RANK + ROPE_DIM)
    queries = jnp.concatenate([mapped_output[..., :KV_RANK], rotate(mapped_output[..., KV_RANK:], places)], axis=-1).astype(jnp.bfloat16)
    fresh_rows = jnp.concatenate([normalize(key_raw[:, :KV_RANK], gain_key), rotate(key_raw[:, KV_RANK:], places)], axis=-1).astype(jnp.bfloat16)
    fresh_block = fresh_rows.reshape(SEQS, PROPS, KV_RANK + ROPE_DIM)
    updated = jax.vmap(location_rows)(latent_cache, fresh_block, filled)
    queries = lax.optimization_barrier(queries).reshape(SEQS, PROPS, HEADS, KV_RANK + ROPE_DIM)
    keys_all = lax.optimization_barrier(updated)

    def one_block(index_block):
        anchor = index_block * POS_DEV
        key_rows = lax.dynamic_slice_in_dim(keys_all, anchor, POS_DEV, 1)
        locations_held = anchor + jnp.arange(POS_DEV, dtype=jnp.int32)
        slot_index = locations_held[None, :] - filled[:, None]
        onehot = (slot_index[:, :, None] == jnp.arange(PROPS, dtype=jnp.int32)[None, None, :]).astype(jnp.float32)
        return partial_attend(queries, key_rows, slot_index, onehot, reached, w_value)
    maxima, totals, values = lax.map(one_block, jnp.arange(N_KV, dtype=jnp.int32))
    values = lax.optimization_barrier(values)
    attended = combine_parts(maxima, totals, values).astype(jnp.bfloat16).reshape(ROWS, HEADS * V_DIM)
    mixed_raw = jnp.dot(attended, w_out, preferred_element_type=jnp.float32)
    mixed = normalize(mixed_raw, gain_output).astype(jnp.bfloat16)
    return (mixed, updated)
```

```python
import functools

import jax
import jax.numpy as jnp
from jax import lax
from jax.experimental import pallas as pl
from jax.experimental.pallas import tpu as pltpu
from jax.sharding import PartitionSpec as P

NOPE_DIM = 64
LANES = 128

epsilon = 1e-06
rope_base = 10000.0
score_after_mask = -1e30
MESH = pl.DeviceIdType.MESH
HIGHEST = lax.Precision.HIGHEST
VMEM = pl.BlockSpec(memory_space=pltpu.VMEM)


def dot(a, b, precision=None):
    return jnp.dot(a, b, preferred_element_type=jnp.float32, precision=precision)


def dot_nt(a, b, precision=None):
    return lax.dot_general(
        a, b, (((1,), (1,)), ((), ())), preferred_element_type=jnp.float32, precision=precision
    )


def remote(src, dst, send_sem, recv_sem, device_id):
    return pltpu.make_async_remote_copy(
        src_ref=src,
        dst_ref=dst,
        send_sem=send_sem,
        recv_sem=recv_sem,
        device_id=device_id,
        device_id_type=MESH,
    )


def root_mean(values, count):
    return lax.rsqrt(jnp.sum(values * values, axis=-1, keepdims=True) / count + epsilon)


def flip(index, bits):
    out = index
    bit = 1
    while bit <= bits:
        if bits & bit:
            out = out + bit - 2 * bit * lax.rem(lax.div(index, bit), 2)
        bit *= 2
    return out


def iota(shape, axis):
    return lax.broadcasted_iota(jnp.int32, shape, axis)


def row_table(lengths, accepted, parents, freq, rows):
    props, seqs = parents.shape
    spread = (lax.div(iota((seqs, rows), 1), props) == iota((seqs, rows), 0)).astype(jnp.float32)
    owner = lax.div(iota((1, rows), 1), props)
    filled = jnp.zeros((1, rows), jnp.int32)
    for s in range(seqs):
        filled = jnp.where(owner == s, lengths[s] + accepted[s], filled)
    filled = filled.astype(jnp.float32)
    links = dot(parents.astype(jnp.float32), spread, HIGHEST)
    own = lax.rem(iota((props, rows), 1), props) == iota((props, rows), 0)
    link = jnp.sum(jnp.where(own, links, 0.0), axis=0, keepdims=True)
    link = link.astype(jnp.int32)
    base = lax.div(iota((1, rows), 1), props) * props
    above = jnp.where(link < 0, -1, base + link)
    up_index = iota((rows, rows), 0)
    reached = jnp.where((up_index == above) | (up_index == iota((rows, rows), 1)), 1.0, 0.0)
    for repeat in range((props - 1).bit_length()):
        half = reached.astype(jnp.bfloat16)
        reached = jnp.minimum(dot(half, half), 1.0)
    compact = jnp.sum(reached.reshape(seqs, props, rows), axis=0)
    place = filled + jnp.sum(compact, axis=0, keepdims=True) - 1.0
    angles = place * freq
    cosine, sine = jnp.cos(angles), jnp.sin(angles)
    rest = LANES - 4 * freq.shape[0] - props
    table = jnp.concatenate(
        [cosine, cosine, -sine, sine, compact, jnp.zeros((rest, rows), jnp.float32)], axis=0
    )
    return table.T


def compress_kernel(
    n_kv, n_tp, few,
    x_hbm, wq_hbm, wk_hbm, gain_x_hbm, gain_q_hbm, gain_k_hbm, parents_hbm,
    lengths_hbm, accepted_hbm, freq_ref, expand_hbm, cache_hbm,
    q_all, k_all, table_ref, expand_ref, held_ref,
    x_own, wq_own, wk_raw, gain_x, gain_q, gain_k, parents_ref, lengths, accepted, wk_own, x_msg, got_x, got_wq, got_wk, part, got_part, sq_all,
    fetch_s, fetch_c,
    send_x, recv_x, send_w, recv_w, send_s, recv_s, send_p, recv_p,
    send_a, send_y, send_b, recv_q, recv_k,
):
    me_k, me_t = lax.axis_index("kv"), lax.axis_index("tp")
    n_y = n_tp // 2
    me_y, core = lax.div(me_t, 2), lax.rem(me_t, 2)
    mine = me_t * n_kv + me_k
    barrier = pltpu.get_barrier_semaphore()
    everyone = [(dk, dt) for dk in range(n_kv) for dt in range(n_tp) if dk or dt]
    for dk, dt in everyone:
        pl.semaphore_signal(
            barrier, inc=1,
            device_id={"kv": flip(me_k, dk), "tp": flip(me_t, dt)}, device_id_type=MESH,
        )
    small = [
        pltpu.make_async_copy(src, dst, fetch_s.at[n])
        for n, (src, dst) in enumerate(
            (
                (x_hbm, x_own), (gain_x_hbm, gain_x), (lengths_hbm, lengths),
                (accepted_hbm, accepted), (parents_hbm, parents_ref), (wk_hbm, wk_raw),
                (wq_hbm, wq_own), (gain_q_hbm, gain_q), (gain_k_hbm, gain_k),
            )
        )
    ]
    for copy in small:
        copy.start()
    big = [pltpu.make_async_copy(expand_hbm, expand_ref, fetch_s.at[9])] + [
        pltpu.make_async_copy(cache_hbm.at[s], held_ref.at[s], fetch_c.at[s])
        for s in range(cache_hbm.shape[0])
    ]
    for copy in small:
        copy.wait()

    features, rows = x_own.shape
    q_rank, kv_rank = gain_q.shape[-1], gain_k.shape[-1]
    whole, wide = wk_raw.shape[1], wk_own.shape[1]
    each, half = part.shape[1], x_msg.shape[1]
    raw = x_own[...].astype(jnp.float32)
    squares = jnp.sum(raw * raw, axis=0, keepdims=True)
    sq_all[mine] = jnp.zeros_like(sq_all[0])
    for n in range(rows // LANES):
        sq_all[mine, n : n + 1, :] = squares[:, n * LANES : (n + 1) * LANES]
    scaled = raw.T * gain_x[...].astype(jnp.float32)[None]
    for y in range(n_y):
        for n in range(2):
            blocks = []
            for j in range(n_kv // 2):
                start = (y * n_kv + n * (n_kv // 2) + j) * few
                blocks.append(scaled[start : start + few])
                if each > few:
                    blocks.append(jnp.zeros((each - few, features), jnp.float32))
            if each == few:
                start = (y * n_kv + n * (n_kv // 2)) * few
                blocks = [scaled[start : start + half]]
            value = jnp.concatenate(blocks, axis=0).astype(jnp.bfloat16)
            x_msg[y, :, n * features : (n + 1) * features] = value
    wk_own[...] = jnp.zeros_like(wk_own)
    wk_own[:, :whole] = wk_raw[...]
    pl.semaphore_wait(barrier, n_kv * n_tp - 1)

    def role(c):
        sends = []

        def start(*args):
            copy = remote(*args)
            copy.start()
            sends.append(copy)

        w_own, got_w, width = (wq_own, got_wq, q_rank) if c == 0 else (wk_own, got_wk, wide)
        for dt in reversed(range(1, n_tp)):
            peer = flip(me_t, dt)
            theirs, land = (wq_own, got_wq) if (c ^ dt) % 2 == 0 else (wk_own, got_wk)
            start(theirs, land.at[me_t], send_w.at[dt], recv_w.at[me_t], {"tp": peer})
            start(
                x_msg.at[lax.div(peer, 2)], got_x.at[me_t], send_x.at[dt], recv_x.at[me_t],
                {"tp": peer},
            )
        for n, (dk, dt) in enumerate(everyone):
            start(
                sq_all.at[mine], sq_all.at[mine], send_s.at[n], recv_s.at[mine],
                {"kv": flip(me_k, dk), "tp": flip(me_t, dt)},
            )
        for copy in big:
            copy.start()
        table_ref[:rows] = row_table(
            lengths, accepted, parents_ref[...], freq_ref[...], rows
        )

        for dt in range(1, n_tp):
            peer = flip(me_t, dt)
            remote(w_own, got_w.at[peer], send_w.at[dt], recv_w.at[peer], {"tp": peer}).wait_recv()
            remote(
                x_msg.at[0], got_x.at[peer], send_x.at[dt], recv_x.at[peer], {"tp": peer}
            ).wait_recv()
        terms = [(x_msg[me_y], w_own[...])]
        for dt in range(1, n_tp):
            peer = flip(me_t, dt)
            terms.append((got_x[peer], got_w[peer]))
        for n in range(2):
            total = None
            for x, w in terms:
                term = dot(x[:, n * features : (n + 1) * features], w)
                total = term if total is None else total + term
            for j in range(n_kv // 2):
                part[n * (n_kv // 2) + j, :, :width] = total[j * each : (j + 1) * each]

        cut = pl.ds(0, width)
        for dk in reversed(range(1, n_kv)):
            peer = flip(me_k, dk)
            start(
                part.at[peer, :, cut], got_part.at[me_k, :, cut], send_p.at[dk],
                recv_p.at[me_k], {"kv": peer},
            )
        block = me_y * n_kv + me_k
        first = block * few
        for n, (dk, dt) in enumerate(everyone):
            source = flip(me_t, dt) * n_kv + flip(me_k, dk)
            remote(
                sq_all.at[source], sq_all.at[source], send_s.at[n], recv_s.at[source],
                {"kv": flip(me_k, dk), "tp": flip(me_t, dt)},
            ).wait_recv()
        square = sq_all[0]
        for n in range(1, n_kv * n_tp):
            square = square + sq_all[n]
        column = jnp.zeros((each, 1), jnp.float32)
        for n in range(rows // LANES):
            here = iota((each, LANES), 1) + n * LANES == iota((each, LANES), 0) + first
            column = column + jnp.sum(
                jnp.where(here, square[n : n + 1], 0.0), axis=1, keepdims=True
            )
        inverse = lax.rsqrt(column / (n_kv * n_tp * features) + epsilon)
        summed = part[me_k, :, :width]
        for dk in range(1, n_kv):
            peer = flip(me_k, dk)
            remote(
                part.at[peer, :, cut], got_part.at[peer, :, cut], send_p.at[dk],
                recv_p.at[peer], {"kv": peer},
            ).wait_recv()
            summed = summed + got_part[peer, :, :width]
        if c == 0:
            query = summed * inverse
            query = query * root_mean(query, q_rank) * gain_q[...].astype(jnp.float32)[None]
            q_all[block] = query.astype(jnp.bfloat16)
        else:
            latent = summed[:, :kv_rank] * inverse
            latent = latent * root_mean(latent, kv_rank) * gain_k[...].astype(jnp.float32)[None]
            k_all[block, :, :kv_rank] = latent.astype(jnp.bfloat16)
            turn = summed[:, kv_rank:] * inverse
            turn_dim = whole - kv_rank
            lane = iota(turn.shape, 1)
            swapped = jnp.where(
                lane < turn_dim // 2,
                pltpu.roll(turn, LANES - turn_dim // 2, 1),
                pltpu.roll(turn, turn_dim // 2, 1),
            )
            angles = table_ref[pl.ds(first, each), :]
            turned = turn * angles + swapped * pltpu.roll(angles, LANES - turn_dim, 1)
            turned = jnp.where(lane < turn_dim, turned, 0.0)
            k_all[block, :, kv_rank:] = turned.astype(jnp.bfloat16)

        ours, recv_ours = (q_all, recv_q) if c == 0 else (k_all, recv_k)
        other, recv_other = (k_all, recv_k) if c == 0 else (q_all, recv_q)
        sibling = me_t + 1 - 2 * c

        def send(n, sem, device_id):
            start(ours.at[n], ours.at[n], sem, recv_ours.at[n], device_id)

        def landed(buf, n, recv):
            remote(buf.at[n], buf.at[n], send_a.at[0], recv.at[n], {"tp": sibling}).wait_recv()

        for dk in reversed(range(1, n_kv)):
            send(block, send_a.at[dk], {"kv": flip(me_k, dk)})
        for dk in range(n_kv):
            here = me_y * n_kv + flip(me_k, dk)
            if dk:
                landed(ours, here, recv_ours)
            for dy in range(1, n_y):
                send(here, send_y.at[dy * n_kv + dk], {"tp": flip(me_t, 2 * dy)})
            send(here, send_b.at[dk], {"tp": sibling})
        for dy in range(1, n_y):
            for dk in range(n_kv):
                here = flip(me_y, dy) * n_kv + flip(me_k, dk)
                landed(ours, here, recv_ours)
                send(here, send_b.at[dy * n_kv + dk], {"tp": sibling})
        for dy in range(n_y):
            for dk in range(n_kv):
                landed(other, flip(me_y, dy) * n_kv + flip(me_k, dk), recv_other)
        for copy in big:
            copy.wait()
        for copy in sends:
            copy.wait_send()

    for c in range(2):
        pl.when(core == c)(functools.partial(role, c))


def attend_kernel(
    group, lengths_ref, accepted_ref, low_ref, fresh_ref, table_ref, wq_ref, held_in,
    out_hbm, part_ref, stats_ref, held_ref, q_main, q_turn, bias, write,
):
    heads, whole, _ = wq_ref.shape
    seqs, _, span = held_ref.shape
    rank = part_ref.shape[-1]
    turn_dim = whole - rank
    half = turn_dim // 2
    props = q_main.shape[1] // heads
    scale = (NOPE_DIM + turn_dim) ** (-0.5)
    rows = low_ref.shape[0]
    offset = lax.axis_index("kv") * span

    low = low_ref[...]
    cosine = table_ref[:rows, :turn_dim]
    sine = table_ref[:rows, turn_dim : 2 * turn_dim]
    for h in range(heads):
        main = dot_nt(low, wq_ref[h, :rank, :])
        front, back = wq_ref[h, rank : rank + half, :], wq_ref[h, rank + half :, :]
        turn = dot_nt(low, jnp.concatenate([front, back], axis=0))
        swapped = dot_nt(low, jnp.concatenate([back, front], axis=0))
        turned = turn * cosine + swapped * sine
        lines = slice(h * props, (h + 1) * props)
        q_main[:, lines, :] = main.astype(jnp.bfloat16).reshape(seqs, props, rank)
        q_turn[:, lines, :] = turned.astype(jnp.bfloat16).reshape(seqs, props, turn_dim)

    def patch(s, carry):
        rel = lengths_ref[s] + accepted_ref[s] - offset
        lines = pl.ds(pl.multiple_of(s * props, props), props)
        first = lax.shift_right_arithmetic(rel, 7)
        last = lax.shift_right_arithmetic(rel + props - 1, 7)
        for more in range(2):
            chunk = first + more

            @pl.when((chunk >= 0) & (chunk < span // LANES) & (chunk <= last))
            def _():
                start = pl.multiple_of(chunk * LANES, LANES)
                slot = start - rel + iota((props, LANES), 1)
                onehot = (slot == iota((props, LANES), 0)).astype(jnp.float32).astype(jnp.bfloat16)
                placed = lax.dot_general(
                    fresh_ref[lines, :whole], onehot, (((0,), (0,)), ((), ())),
                    preferred_element_type=jnp.float32,
                )
                slots = start - rel + iota(placed.shape, 1)
                old = held_ref[s, :, pl.ds(start, LANES)].astype(jnp.float32)
                new = jnp.where((slots >= 0) & (slots < props), placed, old)
                held_ref[s, :, pl.ds(start, LANES)] = new.astype(jnp.bfloat16)

        return carry

    lax.fori_loop(0, seqs, patch, 0)

    def write_out(s):
        return pltpu.make_async_copy(held_ref.at[s], out_hbm.at[s], write.at[s])

    for s in range(seqs):
        write_out(s).start()

    def step(i, carry):
        for g in range(group):
            s = i * group + g
            rel = lengths_ref[s] + accepted_ref[s] - offset
            lines = pl.ds(pl.multiple_of(s * props, props), props)
            past = iota((props, span), 1) < rel
            bias[g] = jnp.where(past, 0.0, score_after_mask)
            first = lax.shift_right_arithmetic(rel, 7)
            last = lax.shift_right_arithmetic(rel + props - 1, 7)
            for more in range(2):
                chunk = first + more

                @pl.when((chunk >= 0) & (chunk < span // LANES) & (chunk <= last))
                def _():
                    start = pl.multiple_of(chunk * LANES, LANES)
                    slot = start - rel + iota((props, LANES), 1)
                    onehot = slot == iota((props, LANES), 0)
                    onehot = onehot.astype(jnp.float32).astype(jnp.bfloat16)
                    reached = table_ref[lines, 2 * turn_dim : 2 * turn_dim + props]
                    seen = (slot < 0) | (dot(reached.astype(jnp.bfloat16), onehot) > 0.5)
                    bias[g, :, pl.ds(start, LANES)] = jnp.where(seen, 0.0, score_after_mask)

        for g in range(group):
            s = i * group + g
            scores = dot(q_main[s], held_ref[s, :rank, :]) + dot(q_turn[s], held_ref[s, rank:, :])
            masked = scores.reshape(heads, props, span) * scale + bias[g][None]
            top = jnp.max(masked, axis=-1, keepdims=True)
            weights = jnp.exp(masked - jnp.maximum(top, -1e29))
            totals = jnp.sum(weights, axis=-1, keepdims=True)
            prob = weights.astype(jnp.bfloat16).reshape(heads * props, span)
            weighted = dot_nt(prob, held_ref[s, :rank, :]).reshape(heads, props, rank)
            part = (weighted / jnp.maximum(totals, 1.0)).astype(jnp.bfloat16)
            lane = iota((props, LANES), 1)
            stats = jnp.zeros((props, LANES), jnp.float32)
            lines = pl.ds(pl.multiple_of(s * props, props), props)
            for h in range(heads):
                part_ref[h, lines, :] = part[h]
                stats = jnp.where(lane == h, top[h], stats)
                stats = jnp.where(lane == heads + h, totals[h], stats)
            stats_ref[lines, :] = stats
        return carry

    lax.fori_loop(0, seqs // group, step, 0)
    for s in range(seqs):
        write_out(s).wait()


def project_kernel(
    n_kv, n_tp,
    part_ref, stats_ref, wv_ref, w_out_ref, gain_ref, out_ref,
    vals, stat, got_vals, got_stat, attended, raw, got_raw, sums, result,
    send_v, recv_v, send_s, recv_s, send_a, recv_a, send_r, recv_r, send_q, recv_q, send_o, recv_o,
):
    me_k, me_t = lax.axis_index("kv"), lax.axis_index("tp")
    heads, _, _ = part_ref.shape
    v_dim = wv_ref.shape[1]
    kv_peers = [lax.rem(me_k + d, n_kv) for d in range(n_kv)]
    tp_peers = [lax.rem(me_t + d, n_tp) for d in range(n_tp)]
    barrier = pltpu.get_barrier_semaphore()
    for dk in range(n_kv):
        for dt in range(n_tp):
            if dk or dt:
                pl.semaphore_signal(
                    barrier, inc=1,
                    device_id={"kv": kv_peers[dk], "tp": tp_peers[dt]}, device_id_type=MESH,
                )
    sends = []

    each = vals.shape[1]
    line = lax.broadcasted_iota(jnp.int32, (16, LANES), 0)
    lane = lax.broadcasted_iota(jnp.int32, (16, LANES), 1)
    tops = (line < heads) & (lane == line)
    counts = (line >= 8) & (line < 8 + heads) & (lane == line - 8 + heads)
    pick = jnp.where(tops | counts, 1.0, 0.0)
    values = jnp.concatenate([dot_nt(part_ref[h], wv_ref[h]) for h in range(heads)], axis=1)
    for j in range(n_kv):
        vals[j] = values[j * each : (j + 1) * each].astype(jnp.bfloat16)
        stat[j] = dot_nt(pick, stats_ref[j * each : (j + 1) * each, :], HIGHEST)
    pl.semaphore_wait(barrier, n_kv * n_tp - 1)

    def exchange(axis, peers, src_of, dst, own, send_sem, recv_sem):
        for d in range(1, len(peers)):
            copy = remote(
                src_of(peers[d]), dst.at[own], send_sem.at[d], recv_sem.at[own], {axis: peers[d]}
            )
            copy.start()
            sends.append(copy)

    def arrived(axis, peers, d, src_of, dst, send_sem, recv_sem):
        remote(
            src_of(peers[d]), dst.at[peers[d]], send_sem.at[d], recv_sem.at[peers[d]],
            {axis: peers[d]},
        ).wait_recv()

    exchange("kv", kv_peers, lambda p: stat.at[p], got_stat, me_k, send_s, recv_s)
    exchange("kv", kv_peers, lambda p: vals.at[p], got_vals, me_k, send_v, recv_v)
    for d in range(1, n_kv):
        arrived("kv", kv_peers, d, lambda p: stat.at[p], got_stat, send_s, recv_s)
    all_stats = [stat[me_k]] + [got_stat[p] for p in kv_peers[1:]]
    largest = all_stats[0][:8]
    for one in all_stats[1:]:
        largest = jnp.maximum(largest, one[:8])
    shares = jnp.concatenate([one[8:] * jnp.exp(one[:8] - largest) for one in all_stats], axis=0)
    turn_eye = lax.broadcasted_iota(jnp.int32, (each, each), 0) == lax.broadcasted_iota(
        jnp.int32, (each, each), 1
    )
    shares = dot_nt(turn_eye.astype(jnp.float32), shares, HIGHEST)
    wide = lax.broadcasted_iota(jnp.int32, (each, heads * v_dim), 1)

    def spread(d):
        out = shares[:, 8 * d : 8 * d + 1]
        for h in range(1, heads):
            out = jnp.where(wide >= h * v_dim, shares[:, 8 * d + h : 8 * d + h + 1], out)
        return jnp.broadcast_to(out, wide.shape)

    summed = None
    for d in range(n_kv):
        share = spread(d)
        if d:
            arrived("kv", kv_peers, d, lambda p: vals.at[p], got_vals, send_v, recv_v)
        block = got_vals[kv_peers[d]] if d else vals[me_k]
        term = share * block.astype(jnp.float32)
        summed = term if summed is None else summed + term
        weight = share if d == 0 else weight + share
    attended[me_k] = (summed / weight).astype(jnp.bfloat16)
    exchange("kv", kv_peers, lambda p: attended.at[me_k], attended, me_k, send_a, recv_a)
    for d in range(1, n_kv):
        arrived("kv", kv_peers, d, lambda p: attended.at[p], attended, send_a, recv_a)

    lines = jnp.concatenate([attended[j].astype(jnp.float32) for j in range(n_kv)], axis=0)
    lines = dot(lines.astype(jnp.bfloat16), w_out_ref[...])
    share_rows, cols = raw.shape[1:]
    for t in range(n_tp):
        raw[t] = lines[t * share_rows : (t + 1) * share_rows].astype(jnp.bfloat16)
    exchange("tp", tp_peers, lambda p: raw.at[p], got_raw, me_t, send_r, recv_r)
    mixed = raw[me_t].astype(jnp.float32)
    for d in range(1, n_tp):
        arrived("tp", tp_peers, d, lambda p: raw.at[p], got_raw, send_r, recv_r)
        mixed = mixed + got_raw[tp_peers[d]].astype(jnp.float32)
    result[me_t] = mixed.astype(jnp.bfloat16)
    exchange("tp", tp_peers, lambda p: result.at[me_t], result, me_t, send_o, recv_o)
    mine = me_t * n_kv + me_k
    sums[mine] = dot_nt(jnp.ones((8, cols), jnp.float32), mixed * mixed, HIGHEST)
    everyone = [(dk, dt) for dt in range(n_tp) for dk in range(n_kv) if dk or dt]
    for n, (dk, dt) in enumerate(everyone):
        copy = remote(
            sums.at[mine], sums.at[mine], send_q.at[n], recv_q.at[mine],
            {"kv": kv_peers[dk], "tp": tp_peers[dt]},
        )
        copy.start()
        sends.append(copy)
    for n, (dk, dt) in enumerate(everyone):
        source = tp_peers[dt] * n_kv + kv_peers[dk]
        remote(
            sums.at[source], sums.at[source], send_q.at[n], recv_q.at[source],
            {"kv": kv_peers[dk], "tp": tp_peers[dt]},
        ).wait_recv()
    eye = iota((share_rows, share_rows), 0) == iota((share_rows, share_rows), 1)
    for d in range(1, n_tp):
        arrived("tp", tp_peers, d, lambda p: result.at[p], result, send_o, recv_o)
    for t in range(n_tp):
        square = sums[t * n_kv]
        for j in range(1, n_kv):
            square = square + sums[t * n_kv + j]
        norm = lax.rsqrt(square / (cols * n_kv) + epsilon)
        column = jnp.sum(jnp.where(eye, norm[:1], 0.0), axis=1, keepdims=True)
        out_ref[t] = (result[t].astype(jnp.float32) * column * gain_ref[...]).astype(jnp.bfloat16)
    for copy in sends:
        copy.wait_send()


def up(value, to):
    return -(-value // to) * to


def local(
    n_kv,
    n_tp,
    activations,
    latent_cache,
    lengths,
    accepted,
    parents,
    w_query_down,
    w_key_down,
    gain_input,
    gain_query,
    gain_key,
    w_query,
    w_value,
    w_out,
    gain_output,
):
    bf16, f32 = jnp.bfloat16, jnp.float32
    seqs, props = parents.shape
    rows, features = activations.shape
    heads = w_query.shape[1]
    q_rank, kv_rank = gain_query.shape[0], gain_key.shape[0]
    whole = latent_cache.shape[-1]
    turn_dim = whole - kv_rank
    half = turn_dim // 2
    span = latent_cache.shape[1]
    v_dim = w_value.shape[-1]
    cols = w_out.shape[1]
    n_dev = n_kv * n_tp
    me_t = lax.axis_index("tp")

    n_y = n_tp // 2
    blocks = n_y * n_kv
    few = rows // blocks
    each = up(few, 8)
    wide = up(whole, LANES)
    frequency = rope_base ** (-jnp.arange(half, dtype=f32) / half)
    dma = pltpu.SemaphoreType.DMA
    hbm = pl.BlockSpec(memory_space=pl.ANY)
    far = lambda array: pltpu.with_memory_space_constraint(array, pltpu.HBM)
    q_all, k_all, table, expand, held = pl.pallas_call(
        functools.partial(compress_kernel, n_kv, n_tp, few),
        name="compress",
        out_shape=(
            jax.ShapeDtypeStruct((blocks, each, q_rank), bf16),
            jax.ShapeDtypeStruct((blocks, each, wide), bf16),
            jax.ShapeDtypeStruct((rows + 8, LANES), f32),
            pltpu.VMEM((heads, whole, q_rank), bf16),
            pltpu.VMEM((seqs, whole, span), bf16),
        ),
        in_specs=[hbm] * 9 + [VMEM] + [hbm] * 2,
        out_specs=(VMEM,) * 5,
        scratch_shapes=[
            pltpu.VMEM((features, rows), bf16),
            pltpu.VMEM((features, q_rank), bf16),
            pltpu.VMEM((features, whole), bf16),
            pltpu.VMEM((features,), bf16),
            pltpu.VMEM((q_rank,), bf16),
            pltpu.VMEM((kv_rank,), bf16),
            pltpu.VMEM((props, seqs), jnp.int32),
            pltpu.SMEM((seqs,), jnp.int32),
            pltpu.SMEM((seqs,), jnp.int32),
            pltpu.VMEM((features, wide), bf16),
            pltpu.VMEM((n_y, n_kv * each // 2, 2 * features), bf16),
            pltpu.VMEM((n_tp, n_kv * each // 2, 2 * features), bf16),
            pltpu.VMEM((n_tp, features, q_rank), bf16),
            pltpu.VMEM((n_tp, features, wide), bf16),
            pltpu.VMEM((n_kv, each, max(q_rank, wide)), f32),
            pltpu.VMEM((n_kv, each, max(q_rank, wide)), f32),
            pltpu.VMEM((n_dev, 8, LANES), f32),
            dma((10,)), dma((seqs,)),
            dma((n_tp,)), dma((n_tp,)), dma((n_tp,)), dma((n_tp,)),
            dma((n_dev,)), dma((n_dev,)), dma((n_kv,)), dma((n_kv,)),
            dma((n_kv,)), dma((blocks,)), dma((blocks,)), dma((blocks,)), dma((blocks,)),
        ],
        compiler_params=pltpu.CompilerParams(
            collective_id=0, has_side_effects=True, vmem_limit_bytes=20 * 1024 * 1024
        ),
    )(
        far(activations.T), far(w_query_down), far(w_key_down),
        far(gain_input), far(gain_query), far(gain_key), far(parents.T),
        far(lengths), far(accepted), frequency[:, None],
        far(w_query.transpose(1, 2, 0)), far(latent_cache.transpose(0, 2, 1)),
    )
    query_low = q_all[:, :few].reshape(rows, q_rank)
    fresh = k_all[:, :few].reshape(rows, wide)

    group = next(g for g in (3, 2, 1) if seqs % g == 0)
    smem = pl.BlockSpec(memory_space=pltpu.SMEM)
    updated, part, stats, _ = pl.pallas_call(
        functools.partial(attend_kernel, group),
        name="attend",
        out_shape=(
            jax.ShapeDtypeStruct((seqs, whole, span), bf16),
            jax.ShapeDtypeStruct((heads, rows, kv_rank), bf16),
            jax.ShapeDtypeStruct((rows, LANES), f32),
            pltpu.VMEM((seqs, whole, span), bf16),
        ),
        in_specs=[smem] * 2 + [VMEM] * 5,
        out_specs=(hbm, VMEM, VMEM, VMEM),
        scratch_shapes=[
            pltpu.VMEM((seqs, heads * props, kv_rank), bf16),
            pltpu.VMEM((seqs, heads * props, turn_dim), bf16),
            pltpu.VMEM((group, props, span), f32),
            dma((seqs,)),
        ],
        input_output_aliases={6: 3},
        compiler_params=pltpu.CompilerParams(vmem_limit_bytes=24 * 1024 * 1024),
    )(
        lengths, accepted, query_low, fresh, table,
        pltpu.with_memory_space_constraint(expand, pltpu.VMEM),
        pltpu.with_memory_space_constraint(held, pltpu.VMEM),
    )

    wv = lax.dynamic_slice_in_dim(w_value.transpose(0, 2, 1), me_t * heads, heads, 0)
    per_kv, per_tp = rows // n_kv, rows // n_tp
    mixed = pl.pallas_call(
        functools.partial(project_kernel, n_kv, n_tp),
        name="project",
        out_shape=jax.ShapeDtypeStruct((n_tp, per_tp, cols), bf16),
        in_specs=[VMEM] * 5,
        out_specs=VMEM,
        scratch_shapes=[
            pltpu.VMEM((n_kv, per_kv, heads * v_dim), bf16),
            pltpu.VMEM((n_kv, 16, per_kv), f32),
            pltpu.VMEM((n_kv, per_kv, heads * v_dim), bf16),
            pltpu.VMEM((n_kv, 16, per_kv), f32),
            pltpu.VMEM((n_kv, per_kv, heads * v_dim), bf16),
            pltpu.VMEM((n_tp, per_tp, cols), bf16),
            pltpu.VMEM((n_tp, per_tp, cols), bf16),
            pltpu.VMEM((n_dev, 8, per_tp), f32),
            pltpu.VMEM((n_tp, per_tp, cols), bf16),
            dma((n_kv,)), dma((n_kv,)), dma((n_kv,)), dma((n_kv,)), dma((n_kv,)), dma((n_kv,)),
            dma((n_tp,)), dma((n_tp,)), dma((n_dev,)), dma((n_dev,)), dma((n_tp,)), dma((n_tp,)),
        ],
        compiler_params=pltpu.CompilerParams(
            collective_id=1, has_side_effects=True, vmem_limit_bytes=32 * 1024 * 1024
        ),
    )(part, stats, wv, w_out, gain_output.astype(f32)[None])
    return (mixed.reshape(rows, cols), updated.transpose(0, 2, 1))


def solution(mesh):
    in_specs = (
        P(None, ("kv", "tp")),
        P(None, "kv", None),
        P(),
        P(),
        P(),
        P(("kv", "tp"), None),
        P(("kv", "tp"), None),
        P(("kv", "tp")),
        P(),
        P(),
        P(None, "tp", None),
        P(),
        P("tp", "kv"),
        P("kv"),
    )
    out_specs = (P(None, "kv"), P(None, "kv", None))
    body = functools.partial(local, mesh.shape["kv"], mesh.shape["tp"])
    return jax.shard_map(body, mesh=mesh, in_specs=in_specs, out_specs=out_specs, check_vma=False)
```

```python
import functools

import jax
import jax.numpy as jnp
from jax import lax
from jax.experimental import pallas as pl
from jax.experimental.pallas import tpu as pltpu
from jax.sharding import PartitionSpec as P

NOPE_DIM = 64
LANES = 128

epsilon = 1e-06
rope_base = 10000.0
score_after_mask = -1e30
MESH = pl.DeviceIdType.MESH
HIGHEST = lax.Precision.HIGHEST
VMEM = pl.BlockSpec(memory_space=pltpu.VMEM)


def dot(a, b, precision=None):
    return jnp.dot(a, b, preferred_element_type=jnp.float32, precision=precision)


def dot_nt(a, b, precision=None):
    return lax.dot_general(
        a, b, (((1,), (1,)), ((), ())), preferred_element_type=jnp.float32, precision=precision
    )


def remote(src, dst, send_sem, recv_sem, device_id):
    return pltpu.make_async_remote_copy(
        src_ref=src,
        dst_ref=dst,
        send_sem=send_sem,
        recv_sem=recv_sem,
        device_id=device_id,
        device_id_type=MESH,
    )


def root_mean(values, count):
    return lax.rsqrt(jnp.sum(values * values, axis=-1, keepdims=True) / count + epsilon)


def flip(index, bits):
    out = index
    bit = 1
    while bit <= bits:
        if bits & bit:
            out = out + bit - 2 * bit * lax.rem(lax.div(index, bit), 2)
        bit *= 2
    return out


def iota(shape, axis):
    return lax.broadcasted_iota(jnp.int32, shape, axis)


def row_table(lengths, accepted, parents, freq, rows):
    props, seqs = parents.shape
    spread = (lax.div(iota((seqs, rows), 1), props) == iota((seqs, rows), 0)).astype(jnp.float32)
    owner = lax.div(iota((1, rows), 1), props)
    filled = jnp.zeros((1, rows), jnp.int32)
    for s in range(seqs):
        filled = jnp.where(owner == s, lengths[s] + accepted[s], filled)
    filled = filled.astype(jnp.float32)
    links = dot(parents.astype(jnp.float32), spread, HIGHEST)
    own = lax.rem(iota((props, rows), 1), props) == iota((props, rows), 0)
    link = jnp.sum(jnp.where(own, links, 0.0), axis=0, keepdims=True)
    link = link.astype(jnp.int32)
    base = lax.div(iota((1, rows), 1), props) * props
    above = jnp.where(link < 0, -1, base + link)
    up_index = iota((rows, rows), 0)
    reached = jnp.where((up_index == above) | (up_index == iota((rows, rows), 1)), 1.0, 0.0)
    for repeat in range((props - 1).bit_length()):
        half = reached.astype(jnp.bfloat16)
        reached = jnp.minimum(dot(half, half), 1.0)
    compact = jnp.sum(reached.reshape(seqs, props, rows), axis=0)
    place = filled + jnp.sum(compact, axis=0, keepdims=True) - 1.0
    angles = place * freq
    cosine, sine = jnp.cos(angles), jnp.sin(angles)
    rest = LANES - 4 * freq.shape[0] - props
    table = jnp.concatenate(
        [cosine, cosine, -sine, sine, compact, jnp.zeros((rest, rows), jnp.float32)], axis=0
    )
    return table.T


def compress_kernel(
    n_kv, n_tp, few,
    x_hbm, wq_hbm, wk_hbm, gain_x_hbm, gain_q_hbm, gain_k_hbm, parents_hbm,
    lengths_hbm, accepted_hbm, freq_ref, expand_hbm, cache_hbm,
    q_all, k_all, table_ref, expand_ref, held_ref,
    x_own, wq_own, wk_raw, gain_x, gain_q, gain_k, parents_ref, lengths, accepted, wk_own, x_msg, got_x, got_wq, got_wk, part, got_part, sq_all,
    fetch_s, fetch_c,
    send_x, recv_x, send_w, recv_w, send_s, recv_s, send_p, recv_p,
    send_a, send_y, send_b, recv_q, recv_k,
):
    me_k, me_t = lax.axis_index("kv"), lax.axis_index("tp")
    n_y = n_tp // 2
    me_y, core = lax.div(me_t, 2), lax.rem(me_t, 2)
    mine = me_t * n_kv + me_k
    barrier = pltpu.get_barrier_semaphore()
    everyone = [(dk, dt) for dk in range(n_kv) for dt in range(n_tp) if dk or dt]
    for dk, dt in everyone:
        pl.semaphore_signal(
            barrier, inc=1,
            device_id={"kv": flip(me_k, dk), "tp": flip(me_t, dt)}, device_id_type=MESH,
        )
    small = [
        pltpu.make_async_copy(src, dst, fetch_s.at[n])
        for n, (src, dst) in enumerate(
            (
                (x_hbm, x_own), (gain_x_hbm, gain_x), (lengths_hbm, lengths),
                (accepted_hbm, accepted), (parents_hbm, parents_ref), (wk_hbm, wk_raw),
                (wq_hbm, wq_own), (gain_q_hbm, gain_q), (gain_k_hbm, gain_k),
            )
        )
    ]
    for copy in small:
        copy.start()
    big = [pltpu.make_async_copy(expand_hbm, expand_ref, fetch_s.at[9])] + [
        pltpu.make_async_copy(cache_hbm.at[s], held_ref.at[s], fetch_c.at[s])
        for s in range(cache_hbm.shape[0])
    ]
    for copy in small:
        copy.wait()

    features, rows = x_own.shape
    q_rank, kv_rank = gain_q.shape[-1], gain_k.shape[-1]
    whole, wide = wk_raw.shape[1], wk_own.shape[1]
    each, half = part.shape[1], x_msg.shape[1]
    raw = x_own[...].astype(jnp.float32)
    squares = jnp.sum(raw * raw, axis=0, keepdims=True)
    sq_all[mine] = jnp.zeros_like(sq_all[0])
    for n in range(rows // LANES):
        sq_all[mine, n : n + 1, :] = squares[:, n * LANES : (n + 1) * LANES]
    scaled = raw.T * gain_x[...].astype(jnp.float32)[None]
    for y in range(n_y):
        for n in range(2):
            blocks = []
            for j in range(n_kv // 2):
                start = (y * n_kv + n * (n_kv // 2) + j) * few
                blocks.append(scaled[start : start + few])
                if each > few:
                    blocks.append(jnp.zeros((each - few, features), jnp.float32))
            if each == few:
                start = (y * n_kv + n * (n_kv // 2)) * few
                blocks = [scaled[start : start + half]]
            value = jnp.concatenate(blocks, axis=0).astype(jnp.bfloat16)
            x_msg[y, :, n * features : (n + 1) * features] = value
    wk_own[...] = jnp.zeros_like(wk_own)
    wk_own[:, :whole] = wk_raw[...]
    pl.semaphore_wait(barrier, n_kv * n_tp - 1)

    def role(c):
        sends = []

        def start(*args):
            copy = remote(*args)
            copy.start()
            sends.append(copy)

        w_own, got_w, width = (wq_own, got_wq, q_rank) if c == 0 else (wk_own, got_wk, wide)
        for dt in reversed(range(1, n_tp)):
            peer = flip(me_t, dt)
            theirs, land = (wq_own, got_wq) if (c ^ dt) % 2 == 0 else (wk_own, got_wk)
            start(theirs, land.at[me_t], send_w.at[dt], recv_w.at[me_t], {"tp": peer})
            start(
                x_msg.at[lax.div(peer, 2)], got_x.at[me_t], send_x.at[dt], recv_x.at[me_t],
                {"tp": peer},
            )
        for n, (dk, dt) in enumerate(everyone):
            start(
                sq_all.at[mine], sq_all.at[mine], send_s.at[n], recv_s.at[mine],
                {"kv": flip(me_k, dk), "tp": flip(me_t, dt)},
            )
        for copy in big:
            copy.start()
        table_ref[:rows] = row_table(
            lengths, accepted, parents_ref[...], freq_ref[...], rows
        )

        for dt in range(1, n_tp):
            peer = flip(me_t, dt)
            remote(w_own, got_w.at[peer], send_w.at[dt], recv_w.at[peer], {"tp": peer}).wait_recv()
            remote(
                x_msg.at[0], got_x.at[peer], send_x.at[dt], recv_x.at[peer], {"tp": peer}
            ).wait_recv()
        terms = [(x_msg[me_y], w_own[...])]
        for dt in range(1, n_tp):
            peer = flip(me_t, dt)
            terms.append((got_x[peer], got_w[peer]))
        for n in range(2):
            total = None
            for x, w in terms:
                term = dot(x[:, n * features : (n + 1) * features], w)
                total = term if total is None else total + term
            for j in range(n_kv // 2):
                part[n * (n_kv // 2) + j, :, :width] = total[j * each : (j + 1) * each]

        cut = pl.ds(0, width)
        for dk in reversed(range(1, n_kv)):
            peer = flip(me_k, dk)
            start(
                part.at[peer, :, cut], got_part.at[me_k, :, cut], send_p.at[dk],
                recv_p.at[me_k], {"kv": peer},
            )
        block = me_y * n_kv + me_k
        first = block * few
        for n, (dk, dt) in enumerate(everyone):
            source = flip(me_t, dt) * n_kv + flip(me_k, dk)
            remote(
                sq_all.at[source], sq_all.at[source], send_s.at[n], recv_s.at[source],
                {"kv": flip(me_k, dk), "tp": flip(me_t, dt)},
            ).wait_recv()
        square = sq_all[0]
        for n in range(1, n_kv * n_tp):
            square = square + sq_all[n]
        column = jnp.zeros((each, 1), jnp.float32)
        for n in range(rows // LANES):
            here = iota((each, LANES), 1) + n * LANES == iota((each, LANES), 0) + first
            column = column + jnp.sum(
                jnp.where(here, square[n : n + 1], 0.0), axis=1, keepdims=True
            )
        inverse = lax.rsqrt(column / (n_kv * n_tp * features) + epsilon)
        summed = part[me_k, :, :width]
        for dk in range(1, n_kv):
            peer = flip(me_k, dk)
            remote(
                part.at[peer, :, cut], got_part.at[peer, :, cut], send_p.at[dk],
                recv_p.at[peer], {"kv": peer},
            ).wait_recv()
            summed = summed + got_part[peer, :, :width]
        if c == 0:
            query = summed * inverse
            query = query * root_mean(query, q_rank) * gain_q[...].astype(jnp.float32)[None]
            q_all[block] = query.astype(jnp.bfloat16)
        else:
            latent = summed[:, :kv_rank] * inverse
            latent = latent * root_mean(latent, kv_rank) * gain_k[...].astype(jnp.float32)[None]
            k_all[block, :, :kv_rank] = latent.astype(jnp.bfloat16)
            turn = summed[:, kv_rank:] * inverse
            turn_dim = whole - kv_rank
            lane = iota(turn.shape, 1)
            swapped = jnp.where(
                lane < turn_dim // 2,
                pltpu.roll(turn, LANES - turn_dim // 2, 1),
                pltpu.roll(turn, turn_dim // 2, 1),
            )
            angles = table_ref[pl.ds(first, each), :]
            turned = turn * angles + swapped * pltpu.roll(angles, LANES - turn_dim, 1)
            turned = jnp.where(lane < turn_dim, turned, 0.0)
            k_all[block, :, kv_rank:] = turned.astype(jnp.bfloat16)

        ours, recv_ours = (q_all, recv_q) if c == 0 else (k_all, recv_k)
        other, recv_other = (k_all, recv_k) if c == 0 else (q_all, recv_q)
        sibling = me_t + 1 - 2 * c

        def send(n, sem, device_id):
            start(ours.at[n], ours.at[n], sem, recv_ours.at[n], device_id)

        def landed(buf, n, recv):
            remote(buf.at[n], buf.at[n], send_a.at[0], recv.at[n], {"tp": sibling}).wait_recv()

        for dk in reversed(range(1, n_kv)):
            send(block, send_a.at[dk], {"kv": flip(me_k, dk)})
        for dk in range(n_kv):
            here = me_y * n_kv + flip(me_k, dk)
            if dk:
                landed(ours, here, recv_ours)
            for dy in range(1, n_y):
                send(here, send_y.at[dy * n_kv + dk], {"tp": flip(me_t, 2 * dy)})
            send(here, send_b.at[dk], {"tp": sibling})
        for dy in range(1, n_y):
            for dk in range(n_kv):
                here = flip(me_y, dy) * n_kv + flip(me_k, dk)
                landed(ours, here, recv_ours)
                send(here, send_b.at[dy * n_kv + dk], {"tp": sibling})
        for dy in range(n_y):
            for dk in range(n_kv):
                landed(other, flip(me_y, dy) * n_kv + flip(me_k, dk), recv_other)
        for copy in big:
            copy.wait()
        for copy in sends:
            copy.wait_send()

    for c in range(2):
        pl.when(core == c)(functools.partial(role, c))


def attend_kernel(
    group, lengths_ref, accepted_ref, low_ref, fresh_ref, table_ref, wq_ref, held_in,
    out_hbm, part_ref, stats_ref, held_ref, q_main, q_turn, bias, turned_ref, write,
):
    heads, whole, _ = wq_ref.shape
    seqs, _, span = held_ref.shape
    rank = part_ref.shape[-1]
    turn_dim = whole - rank
    half = turn_dim // 2
    props = q_main.shape[1] // heads
    power = (NOPE_DIM + turn_dim) ** (-0.5) * 1.4426950408889634
    rows = low_ref.shape[0]
    offset = lax.axis_index("kv") * span

    low = low_ref[...]
    cosine = table_ref[:rows, :turn_dim]
    sine = table_ref[:rows, turn_dim : 2 * turn_dim]
    for h in range(heads):
        main = dot_nt(low, wq_ref[h, :rank, :])
        front, back = wq_ref[h, rank : rank + half, :], wq_ref[h, rank + half :, :]
        turn = dot_nt(low, jnp.concatenate([front, back], axis=0))
        swapped = dot_nt(low, jnp.concatenate([back, front], axis=0))
        turned = turn * cosine + swapped * sine
        lines = slice(h * props, (h + 1) * props)
        q_main[:, lines, :] = main.astype(jnp.bfloat16).reshape(seqs, props, rank)
        q_turn[:, lines, :] = turned.astype(jnp.bfloat16).reshape(seqs, props, turn_dim)

    def patch(s, carry):
        rel = lengths_ref[s] + accepted_ref[s] - offset
        lines = pl.ds(pl.multiple_of(s * props, props), props)
        past = iota((props, span), 1) < rel
        bias[s] = jnp.where(past, 0.0, score_after_mask * 1.5)
        first = lax.shift_right_arithmetic(rel, 7)
        last = lax.shift_right_arithmetic(rel + props - 1, 7)
        for more in range(2):
            chunk = first + more

            @pl.when((chunk >= 0) & (chunk < span // LANES) & (chunk <= last))
            def _():
                start = pl.multiple_of(chunk * LANES, LANES)
                slot = start - rel + iota((props, LANES), 1)
                onehot = (slot == iota((props, LANES), 0)).astype(jnp.float32).astype(jnp.bfloat16)
                reached = table_ref[lines, 2 * turn_dim : 2 * turn_dim + props]
                seen = (slot < 0) | (dot(reached.astype(jnp.bfloat16), onehot) > 0.5)
                bias[s, :, pl.ds(start, LANES)] = jnp.where(seen, 0.0, score_after_mask * 1.5)
                placed = lax.dot_general(
                    fresh_ref[lines, :whole], onehot, (((0,), (0,)), ((), ())),
                    preferred_element_type=jnp.float32,
                )
                slots = start - rel + iota(placed.shape, 1)
                old = held_ref[s, :, pl.ds(start, LANES)].astype(jnp.float32)
                new = jnp.where((slots >= 0) & (slots < props), placed, old)
                held_ref[s, :, pl.ds(start, LANES)] = new.astype(jnp.bfloat16)

        return carry

    lax.fori_loop(0, seqs, patch, 0)

    def write_out(s):
        return pltpu.make_async_copy(held_ref.at[s], out_hbm.at[s], write.at[s])

    for s in range(seqs):
        write_out(s).start()

    def step(i, carry):
        def score_of(s):
            scores = dot(q_main[s], held_ref[s, :rank, :]) + dot(q_turn[s], held_ref[s, rank:, :])
            return scores.reshape(heads, props, span) * power + bias[s][None]

        def finish(s, g, masked):
            top = jnp.max(masked, axis=-1, keepdims=True)
            weights = jnp.exp2(masked - jnp.maximum(top, -1e29))
            totals = jnp.sum(weights, axis=-1, keepdims=True)
            prob = weights.astype(jnp.bfloat16).reshape(heads * props, span)
            turned_ref[g] = held_ref[s, :rank, :].T
            weighted = dot(prob, turned_ref[g]).reshape(heads, props, rank)
            top = jnp.maximum(top * 0.6931471805599453, score_after_mask)
            part = (weighted / jnp.maximum(totals, 1.0)).astype(jnp.bfloat16)
            lane = iota((props, LANES), 1)
            stats = jnp.zeros((props, LANES), jnp.float32)
            lines = pl.ds(pl.multiple_of(s * props, props), props)
            for h in range(heads):
                part_ref[h, lines, :] = part[h]
                stats = jnp.where(lane == h, top[h], stats)
                stats = jnp.where(lane == heads + h, totals[h], stats)
            stats_ref[lines, :] = stats

        maskeds = [score_of(i * group + g) for g in range(group)]
        for g in range(group):
            finish(i * group + g, g, maskeds[g])
        return carry

    lax.fori_loop(0, seqs // group, step, 0)
    for s in range(seqs):
        write_out(s).wait()


def project_kernel(
    n_kv, n_tp,
    part_ref, stats_ref, wv_ref, w_out_ref, gain_ref, out_ref,
    vals, stat, got_vals, got_stat, attended, raw, got_raw, sums, result,
    send_v, recv_v, send_s, recv_s, send_a, recv_a, send_r, recv_r, send_q, recv_q, send_o, recv_o,
):
    me_k, me_t = lax.axis_index("kv"), lax.axis_index("tp")
    mine = me_t * n_kv + me_k
    heads, _, _ = part_ref.shape
    v_dim = wv_ref.shape[1]
    pieces, _, each, _ = vals.shape
    kv_peers = [flip(me_k, d) for d in range(n_kv)]
    tp_peers = [flip(me_t, d) for d in range(n_tp)]
    barrier = pltpu.get_barrier_semaphore()
    everyone = [(dk, dt) for dt in range(n_tp) for dk in range(n_kv) if dk or dt]
    for dk, dt in everyone:
        pl.semaphore_signal(
            barrier, inc=1,
            device_id={"kv": kv_peers[dk], "tp": tp_peers[dt]}, device_id_type=MESH,
        )
    sends = []

    line, lane = iota((8, LANES), 0), iota((8, LANES), 1)
    tops = (line < heads) & (lane == line)
    counts = (line >= 4) & (line < 4 + heads) & (lane == line - 4 + heads)
    pick = jnp.where(tops | counts, 1.0, 0.0)
    values = jnp.concatenate([dot_nt(part_ref[h], wv_ref[h]) for h in range(heads)], axis=1)
    for c in range(pieces):
        for j in range(n_kv):
            lines = slice((j * pieces + c) * each, (j * pieces + c + 1) * each)
            vals[c, j] = values[lines].astype(jnp.bfloat16)
            stat[c, j] = dot_nt(pick, stats_ref[lines, :], HIGHEST)
    pl.semaphore_wait(barrier, n_kv * n_tp - 1)

    def exchange(c, axis, peers, src_of, dst, own, send_sem, recv_sem):
        for d in reversed(range(1, len(peers))):
            copy = remote(
                src_of(peers[d]), dst.at[c, own], send_sem.at[c, d], recv_sem.at[c, own],
                {axis: peers[d]},
            )
            copy.start()
            sends.append(copy)

    def arrived(c, axis, peers, d, dst, send_sem, recv_sem):
        here = dst.at[c, peers[d]]
        remote(
            here, here, send_sem.at[c, d], recv_sem.at[c, peers[d]], {axis: peers[d]}
        ).wait_recv()

    for c in range(pieces):
        exchange(c, "kv", kv_peers, lambda p: stat.at[c, p], got_stat, me_k, send_s, recv_s)
        exchange(c, "kv", kv_peers, lambda p: vals.at[c, p], got_vals, me_k, send_v, recv_v)

    eye = iota((each, each), 0) == iota((each, each), 1)
    wide = iota((each, heads * v_dim), 1)
    for c in range(pieces):
        for d in range(1, n_kv):
            arrived(c, "kv", kv_peers, d, got_stat, send_s, recv_s)
        all_stats = [stat[c, me_k]] + [got_stat[c, p] for p in kv_peers[1:]]
        largest = all_stats[0]
        for one in all_stats[1:]:
            largest = jnp.maximum(largest, one)
        largest = largest[:4]
        shares = [one[4:] * jnp.exp(one[:4] - largest) for one in all_stats]
        shares = dot_nt(eye.astype(jnp.float32), jnp.concatenate(shares, axis=0), HIGHEST)
        summed = None
        for d in range(n_kv):
            share = shares[:, 4 * d : 4 * d + 1]
            for h in range(1, heads):
                share = jnp.where(wide >= h * v_dim, shares[:, 4 * d + h : 4 * d + h + 1], share)
            share = jnp.broadcast_to(share, wide.shape)
            if d:
                arrived(c, "kv", kv_peers, d, got_vals, send_v, recv_v)
            block = got_vals[c, kv_peers[d]] if d else vals[c, me_k]
            term = share * block.astype(jnp.float32)
            summed = term if summed is None else summed + term
            weight = share if d == 0 else weight + share
        attended[c, me_k] = (summed / weight).astype(jnp.bfloat16)
        exchange(
            c, "kv", kv_peers, lambda p: attended.at[c, me_k], attended, me_k, send_a, recv_a
        )

    share_rows, cols = raw.shape[2:]
    for c in range(pieces):
        for d in range(1, n_kv):
            arrived(c, "kv", kv_peers, d, attended, send_a, recv_a)
        lines = [attended[c, j].astype(jnp.float32) for j in range(n_kv)]
        lines = dot(jnp.concatenate(lines, axis=0).astype(jnp.bfloat16), w_out_ref[...])
        for t in range(n_tp):
            raw[c, t] = lines[t * share_rows : (t + 1) * share_rows].astype(jnp.bfloat16)
        exchange(c, "tp", tp_peers, lambda p: raw.at[c, p], got_raw, me_t, send_r, recv_r)

    for c in range(pieces):
        mixed = raw[c, me_t].astype(jnp.float32)
        for d in range(1, n_tp):
            arrived(c, "tp", tp_peers, d, got_raw, send_r, recv_r)
            mixed = mixed + got_raw[c, tp_peers[d]].astype(jnp.float32)
        result[c, me_t] = mixed.astype(jnp.bfloat16)
        sums[c, mine] = dot_nt(jnp.ones((8, cols), jnp.float32), mixed * mixed, HIGHEST)
        for n, (dk, dt) in reversed(list(enumerate(everyone))):
            copy = remote(
                sums.at[c, mine], sums.at[c, mine], send_q.at[c, n], recv_q.at[c, mine],
                {"kv": kv_peers[dk], "tp": tp_peers[dt]},
            )
            copy.start()
            sends.append(copy)
        exchange(c, "tp", tp_peers, lambda p: result.at[c, me_t], result, me_t, send_o, recv_o)

    eye = iota((share_rows, share_rows), 0) == iota((share_rows, share_rows), 1)
    for c in range(pieces):
        for d in range(1, n_tp):
            arrived(c, "tp", tp_peers, d, result, send_o, recv_o)
        for n, (dk, dt) in enumerate(everyone):
            source = tp_peers[dt] * n_kv + kv_peers[dk]
            here = sums.at[c, source]
            remote(
                here, here, send_q.at[c, n], recv_q.at[c, source],
                {"kv": kv_peers[dk], "tp": tp_peers[dt]},
            ).wait_recv()
        for t in range(n_tp):
            square = sums[c, t * n_kv]
            for j in range(1, n_kv):
                square = square + sums[c, t * n_kv + j]
            norm = lax.rsqrt(square / (cols * n_kv) + epsilon)
            column = jnp.sum(jnp.where(eye, norm[:1], 0.0), axis=1, keepdims=True)
            rows = result[c, t].astype(jnp.float32) * column * gain_ref[...]
            for o in range(share_rows // each):
                out_ref[t, o, c] = rows[o * each : (o + 1) * each].astype(jnp.bfloat16)
    for copy in sends:
        copy.wait_send()


def up(value, to):
    return -(-value // to) * to


def local(
    n_kv,
    n_tp,
    activations,
    latent_cache,
    lengths,
    accepted,
    parents,
    w_query_down,
    w_key_down,
    gain_input,
    gain_query,
    gain_key,
    w_query,
    w_value,
    w_out,
    gain_output,
):
    bf16, f32 = jnp.bfloat16, jnp.float32
    seqs, props = parents.shape
    rows, features = activations.shape
    heads = w_query.shape[1]
    q_rank, kv_rank = gain_query.shape[0], gain_key.shape[0]
    whole = latent_cache.shape[-1]
    turn_dim = whole - kv_rank
    half = turn_dim // 2
    span = latent_cache.shape[1]
    v_dim = w_value.shape[-1]
    cols = w_out.shape[1]
    n_dev = n_kv * n_tp
    me_t = lax.axis_index("tp")

    n_y = n_tp // 2
    blocks = n_y * n_kv
    few = rows // blocks
    each = up(few, 8)
    wide = up(whole, LANES)
    frequency = rope_base ** (-jnp.arange(half, dtype=f32) / half)
    dma = pltpu.SemaphoreType.DMA
    hbm = pl.BlockSpec(memory_space=pl.ANY)
    far = lambda array: pltpu.with_memory_space_constraint(array, pltpu.HBM)
    q_all, k_all, table, expand, held = pl.pallas_call(
        functools.partial(compress_kernel, n_kv, n_tp, few),
        name="compress",
        out_shape=(
            jax.ShapeDtypeStruct((blocks, each, q_rank), bf16),
            jax.ShapeDtypeStruct((blocks, each, wide), bf16),
            jax.ShapeDtypeStruct((rows + 8, LANES), f32),
            pltpu.VMEM((heads, whole, q_rank), bf16),
            pltpu.VMEM((seqs, whole, span), bf16),
        ),
        in_specs=[hbm] * 9 + [VMEM] + [hbm] * 2,
        out_specs=(VMEM,) * 5,
        scratch_shapes=[
            pltpu.VMEM((features, rows), bf16),
            pltpu.VMEM((features, q_rank), bf16),
            pltpu.VMEM((features, whole), bf16),
            pltpu.VMEM((features,), bf16),
            pltpu.VMEM((q_rank,), bf16),
            pltpu.VMEM((kv_rank,), bf16),
            pltpu.VMEM((props, seqs), jnp.int32),
            pltpu.SMEM((seqs,), jnp.int32),
            pltpu.SMEM((seqs,), jnp.int32),
            pltpu.VMEM((features, wide), bf16),
            pltpu.VMEM((n_y, n_kv * each // 2, 2 * features), bf16),
            pltpu.VMEM((n_tp, n_kv * each // 2, 2 * features), bf16),
            pltpu.VMEM((n_tp, features, q_rank), bf16),
            pltpu.VMEM((n_tp, features, wide), bf16),
            pltpu.VMEM((n_kv, each, max(q_rank, wide)), f32),
            pltpu.VMEM((n_kv, each, max(q_rank, wide)), f32),
            pltpu.VMEM((n_dev, 8, LANES), f32),
            dma((10,)), dma((seqs,)),
            dma((n_tp,)), dma((n_tp,)), dma((n_tp,)), dma((n_tp,)),
            dma((n_dev,)), dma((n_dev,)), dma((n_kv,)), dma((n_kv,)),
            dma((n_kv,)), dma((blocks,)), dma((blocks,)), dma((blocks,)), dma((blocks,)),
        ],
        compiler_params=pltpu.CompilerParams(
            collective_id=0, has_side_effects=True, vmem_limit_bytes=20 * 1024 * 1024
        ),
    )(
        far(activations.T), far(w_query_down), far(w_key_down),
        far(gain_input), far(gain_query), far(gain_key), far(parents.T),
        far(lengths), far(accepted), frequency[:, None],
        far(w_query.transpose(1, 2, 0)), far(latent_cache.transpose(0, 2, 1)),
    )
    query_low = q_all[:, :few].reshape(rows, q_rank)
    fresh = k_all[:, :few].reshape(rows, wide)

    group = next(g for g in (3, 2, 1) if seqs % g == 0)
    smem = pl.BlockSpec(memory_space=pltpu.SMEM)
    updated, part, stats, _ = pl.pallas_call(
        functools.partial(attend_kernel, group),
        name="attend",
        out_shape=(
            jax.ShapeDtypeStruct((seqs, whole, span), bf16),
            jax.ShapeDtypeStruct((heads, rows, kv_rank), bf16),
            jax.ShapeDtypeStruct((rows, LANES), f32),
            pltpu.VMEM((seqs, whole, span), bf16),
        ),
        in_specs=[smem] * 2 + [VMEM] * 5,
        out_specs=(hbm, VMEM, VMEM, VMEM),
        scratch_shapes=[
            pltpu.VMEM((seqs, heads * props, kv_rank), bf16),
            pltpu.VMEM((seqs, heads * props, turn_dim), bf16),
            pltpu.VMEM((seqs, props, span), f32),
            pltpu.VMEM((group, span, kv_rank), bf16),
            dma((seqs,)),
        ],
        input_output_aliases={6: 3},
        compiler_params=pltpu.CompilerParams(vmem_limit_bytes=24 * 1024 * 1024),
    )(
        lengths, accepted, query_low, fresh, table,
        pltpu.with_memory_space_constraint(expand, pltpu.VMEM),
        pltpu.with_memory_space_constraint(held, pltpu.VMEM),
    )

    wv = lax.dynamic_slice_in_dim(w_value.transpose(0, 2, 1), me_t * heads, heads, 0)
    per_kv, share = rows // n_kv, n_kv // n_tp
    pieces = 1
    lot = per_kv // pieces
    mixed = pl.pallas_call(
        functools.partial(project_kernel, n_kv, n_tp),
        name="project",
        out_shape=jax.ShapeDtypeStruct((n_tp, share, pieces, lot, cols), bf16),
        in_specs=[VMEM] * 5,
        out_specs=VMEM,
        scratch_shapes=[
            pltpu.VMEM((pieces, n_kv, lot, heads * v_dim), bf16),
            pltpu.VMEM((pieces, n_kv, 8, lot), f32),
            pltpu.VMEM((pieces, n_kv, lot, heads * v_dim), bf16),
            pltpu.VMEM((pieces, n_kv, 8, lot), f32),
            pltpu.VMEM((pieces, n_kv, lot, heads * v_dim), bf16),
            pltpu.VMEM((pieces, n_tp, share * lot, cols), bf16),
            pltpu.VMEM((pieces, n_tp, share * lot, cols), bf16),
            pltpu.VMEM((pieces, n_dev, 8, share * lot), f32),
            pltpu.VMEM((pieces, n_tp, share * lot, cols), bf16),
        ]
        + [dma((pieces, n)) for n in (n_kv,) * 6 + (n_tp,) * 2 + (n_dev,) * 2 + (n_tp,) * 2],
        compiler_params=pltpu.CompilerParams(
            collective_id=1, has_side_effects=True, vmem_limit_bytes=32 * 1024 * 1024
        ),
    )(part, stats, wv, w_out, gain_output.astype(f32)[None])
    return (mixed.reshape(rows, cols), updated.transpose(0, 2, 1))


def solution(mesh):
    in_specs = (
        P(None, ("kv", "tp")),
        P(None, "kv", None),
        P(),
        P(),
        P(),
        P(("kv", "tp"), None),
        P(("kv", "tp"), None),
        P(("kv", "tp")),
        P(),
        P(),
        P(None, "tp", None),
        P(),
        P("tp", "kv"),
        P("kv"),
    )
    out_specs = (P(None, "kv"), P(None, "kv", None))
    body = functools.partial(local, mesh.shape["kv"], mesh.shape["tp"])
    return jax.shard_map(body, mesh=mesh, in_specs=in_specs, out_specs=out_specs, check_vma=False)
```

```python
import functools

import jax
import jax.numpy as jnp
from jax import lax
from jax.experimental import pallas as pl
from jax.experimental.pallas import tpu as pltpu
from jax.sharding import PartitionSpec as P

NOPE_DIM = 64
LANES = 128

epsilon = 1e-06
rope_base = 10000.0
score_after_mask = -1e30
MESH = pl.DeviceIdType.MESH
HIGHEST = lax.Precision.HIGHEST
VMEM = pl.BlockSpec(memory_space=pltpu.VMEM)


def dot(a, b, precision=None):
    return jnp.dot(a, b, preferred_element_type=jnp.float32, precision=precision)


def dot_nt(a, b, precision=None):
    return lax.dot_general(
        a, b, (((1,), (1,)), ((), ())), preferred_element_type=jnp.float32, precision=precision
    )


def remote(src, dst, send_sem, recv_sem, device_id):
    return pltpu.make_async_remote_copy(
        src_ref=src,
        dst_ref=dst,
        send_sem=send_sem,
        recv_sem=recv_sem,
        device_id=device_id,
        device_id_type=MESH,
    )


def root_mean(values, count):
    return lax.rsqrt(jnp.sum(values * values, axis=-1, keepdims=True) / count + epsilon)


def flip(index, bits):
    out = index
    bit = 1
    while bit <= bits:
        if bits & bit:
            out = out + bit - 2 * bit * lax.rem(lax.div(index, bit), 2)
        bit *= 2
    return out


def iota(shape, axis):
    return lax.broadcasted_iota(jnp.int32, shape, axis)


def row_table(lengths, accepted, parents, freq, rows):
    props, seqs = parents.shape
    spread = (lax.div(iota((seqs, rows), 1), props) == iota((seqs, rows), 0)).astype(jnp.float32)
    owner = lax.div(iota((1, rows), 1), props)
    filled = jnp.zeros((1, rows), jnp.int32)
    for s in range(seqs):
        filled = jnp.where(owner == s, lengths[s] + accepted[s], filled)
    filled = filled.astype(jnp.float32)
    links = dot(parents.astype(jnp.float32), spread, HIGHEST)
    own = lax.rem(iota((props, rows), 1), props) == iota((props, rows), 0)
    link = jnp.sum(jnp.where(own, links, 0.0), axis=0, keepdims=True)
    link = link.astype(jnp.int32)
    base = lax.div(iota((1, rows), 1), props) * props
    above = jnp.where(link < 0, -1, base + link)
    up_index = iota((rows, rows), 0)
    reached = jnp.where((up_index == above) | (up_index == iota((rows, rows), 1)), 1.0, 0.0)
    for repeat in range((props - 1).bit_length()):
        half = reached.astype(jnp.bfloat16)
        reached = jnp.minimum(dot(half, half), 1.0)
    compact = jnp.sum(reached.reshape(seqs, props, rows), axis=0)
    place = filled + jnp.sum(compact, axis=0, keepdims=True) - 1.0
    angles = place * freq
    cosine, sine = jnp.cos(angles), jnp.sin(angles)
    rest = LANES - 4 * freq.shape[0] - props
    table = jnp.concatenate(
        [cosine, cosine, -sine, sine, compact, jnp.zeros((rest, rows), jnp.float32)], axis=0
    )
    return table.T


def compress_kernel(
    n_kv, n_tp, few,
    x_hbm, wq_hbm, wk_hbm, gain_x_hbm, gain_q_hbm, gain_k_hbm, parents_hbm,
    lengths_hbm, accepted_hbm, freq_ref, expand_hbm, cache_hbm,
    q_all, k_all, table_ref, expand_ref, held_ref,
    x_own, wq_own, wk_raw, gain_x, gain_q, gain_k, parents_ref, lengths, accepted, wk_own, x_msg, got_x, got_wq, got_wk, part_q, got_q, part_k, got_k, sq_tp, sq_kv,
    fetch_s, fetch_c,
    send_x, recv_x, send_w, recv_w, send_s, recv_s, send_z, recv_z, send_p, recv_p,
    send_a, send_y, send_b, recv_q, recv_k,
):
    me_k, me_t = lax.axis_index("kv"), lax.axis_index("tp")
    n_y = n_tp // 2
    me_y, core = lax.div(me_t, 2), lax.rem(me_t, 2)
    barrier = pltpu.get_barrier_semaphore()
    partners = [{"kv": flip(me_k, d)} for d in range(1, n_kv)]
    partners += [{"tp": flip(me_t, d)} for d in range(1, n_tp)]
    for partner in partners:
        pl.semaphore_signal(barrier, inc=1, device_id=partner, device_id_type=MESH)
    small = [
        pltpu.make_async_copy(src, dst, fetch_s.at[n])
        for n, (src, dst) in enumerate(
            (
                (x_hbm, x_own), (gain_x_hbm, gain_x), (lengths_hbm, lengths),
                (accepted_hbm, accepted), (parents_hbm, parents_ref), (wk_hbm, wk_raw),
                (wq_hbm, wq_own), (gain_q_hbm, gain_q), (gain_k_hbm, gain_k),
            )
        )
    ]
    for copy in small:
        copy.start()
    big = [pltpu.make_async_copy(expand_hbm, expand_ref, fetch_s.at[9])] + [
        pltpu.make_async_copy(cache_hbm.at[s], held_ref.at[s], fetch_c.at[s])
        for s in range(cache_hbm.shape[0])
    ]
    for copy in small:
        copy.wait()

    features, rows = x_own.shape
    q_rank, kv_rank = gain_q.shape[-1], gain_k.shape[-1]
    whole, wide = wk_raw.shape[1], wk_own.shape[1]
    each, half = part_q.shape[1], x_msg.shape[1]
    raw = x_own[...].astype(jnp.float32)
    squares = jnp.sum(raw * raw, axis=0, keepdims=True)
    sq_tp[me_t] = jnp.zeros_like(sq_tp[0])
    for n in range(rows // LANES):
        sq_tp[me_t, n : n + 1, :] = squares[:, n * LANES : (n + 1) * LANES]
    scaled = raw.T * gain_x[...].astype(jnp.float32)[None]
    for y in range(n_y):
        for n in range(2):
            blocks = []
            for j in range(n_kv // 2):
                start = (y * n_kv + n * (n_kv // 2) + j) * few
                blocks.append(scaled[start : start + few])
                if each > few:
                    blocks.append(jnp.zeros((each - few, features), jnp.float32))
            if each == few:
                start = (y * n_kv + n * (n_kv // 2)) * few
                blocks = [scaled[start : start + half]]
            value = jnp.concatenate(blocks, axis=0).astype(jnp.bfloat16)
            x_msg[y, :, n * features : (n + 1) * features] = value
    wk_own[...] = jnp.zeros_like(wk_own)
    wk_own[:, :whole] = wk_raw[...]
    pl.semaphore_wait(barrier, len(partners))

    def role(c):
        sends = []

        def start(*args):
            copy = remote(*args)
            copy.start()
            sends.append(copy)

        w_own, got_w = (wq_own, got_wq) if c == 0 else (wk_own, got_wk)
        part, got_part = (part_q, got_q) if c == 0 else (part_k, got_k)
        for dt in reversed(range(1, n_tp)):
            peer = flip(me_t, dt)
            theirs, land = (wq_own, got_wq) if (c ^ dt) % 2 == 0 else (wk_own, got_wk)
            start(theirs, land.at[me_t], send_w.at[dt], recv_w.at[me_t], {"tp": peer})
            start(
                x_msg.at[lax.div(peer, 2)], got_x.at[me_t], send_x.at[dt], recv_x.at[me_t],
                {"tp": peer},
            )
            start(sq_tp.at[me_t], sq_tp.at[me_t], send_s.at[dt], recv_s.at[me_t], {"tp": peer})
        for copy in big:
            copy.start()
        table_ref[:rows] = row_table(
            lengths, accepted, parents_ref[...], freq_ref[...], rows
        )

        for dt in range(1, n_tp):
            peer = flip(me_t, dt)
            remote(w_own, got_w.at[peer], send_w.at[dt], recv_w.at[peer], {"tp": peer}).wait_recv()
            remote(
                x_msg.at[0], got_x.at[peer], send_x.at[dt], recv_x.at[peer], {"tp": peer}
            ).wait_recv()
            remote(
                sq_tp.at[peer], sq_tp.at[peer], send_s.at[dt], recv_s.at[peer], {"tp": peer}
            ).wait_recv()
        square = sq_tp[0]
        for t in range(1, n_tp):
            square = square + sq_tp[t]
        sq_kv[me_k] = square
        terms = [(x_msg[me_y], w_own[...])]
        for dt in range(1, n_tp):
            peer = flip(me_t, dt)
            terms.append((got_x[peer], got_w[peer]))
        for n in range(2):
            total = None
            for x, w in terms:
                term = dot(x[:, n * features : (n + 1) * features], w)
                total = term if total is None else total + term
            for j in range(n_kv // 2):
                part[n * (n_kv // 2) + j] = total[j * each : (j + 1) * each].astype(part.dtype)

        used = pl.ds(0, rows // LANES)
        for dk in reversed(range(1, n_kv)):
            peer = flip(me_k, dk)
            mine = sq_kv.at[me_k, used]
            start(mine, mine, send_z.at[dk], recv_z.at[me_k], {"kv": peer})
        for dk in reversed(range(1, n_kv)):
            peer = flip(me_k, dk)
            start(
                part.at[peer], got_part.at[me_k], send_p.at[dk],
                recv_p.at[me_k], {"kv": peer},
            )
        block = me_y * n_kv + me_k
        first = block * few
        for dk in range(1, n_kv):
            peer = flip(me_k, dk)
            here = sq_kv.at[peer, used]
            remote(here, here, send_z.at[dk], recv_z.at[peer], {"kv": peer}).wait_recv()
        square = sq_kv[0, : rows // LANES]
        for k in range(1, n_kv):
            square = square + sq_kv[k, : rows // LANES]
        column = jnp.zeros((each, 1), jnp.float32)
        for n in range(rows // LANES):
            here = iota((each, LANES), 1) + n * LANES == iota((each, LANES), 0) + first
            column = column + jnp.sum(
                jnp.where(here, square[n : n + 1], 0.0), axis=1, keepdims=True
            )
        inverse = lax.rsqrt(column / (n_kv * n_tp * features) + epsilon)
        summed = part[me_k].astype(jnp.float32)
        for dk in range(1, n_kv):
            peer = flip(me_k, dk)
            remote(
                part.at[peer], got_part.at[peer], send_p.at[dk],
                recv_p.at[peer], {"kv": peer},
            ).wait_recv()
            summed = summed + got_part[peer].astype(jnp.float32)
        if c == 0:
            query = summed * inverse
            query = query * root_mean(query, q_rank) * gain_q[...].astype(jnp.float32)[None]
            q_all[block] = query.astype(jnp.bfloat16)
        else:
            latent = summed[:, :kv_rank] * inverse
            latent = latent * root_mean(latent, kv_rank) * gain_k[...].astype(jnp.float32)[None]
            k_all[block, :, :kv_rank] = latent.astype(jnp.bfloat16)
            turn = summed[:, kv_rank:] * inverse
            turn_dim = whole - kv_rank
            lane = iota(turn.shape, 1)
            swapped = jnp.where(
                lane < turn_dim // 2,
                pltpu.roll(turn, LANES - turn_dim // 2, 1),
                pltpu.roll(turn, turn_dim // 2, 1),
            )
            angles = table_ref[pl.ds(first, each), :]
            turned = turn * angles + swapped * pltpu.roll(angles, LANES - turn_dim, 1)
            turned = jnp.where(lane < turn_dim, turned, 0.0)
            k_all[block, :, kv_rank:] = turned.astype(jnp.bfloat16)

        ours, recv_ours = (q_all, recv_q) if c == 0 else (k_all, recv_k)
        other, recv_other = (k_all, recv_k) if c == 0 else (q_all, recv_q)
        sibling = me_t + 1 - 2 * c

        def send(n, sem, device_id):
            start(ours.at[n], ours.at[n], sem, recv_ours.at[n], device_id)

        def landed(buf, n, recv):
            remote(buf.at[n], buf.at[n], send_a.at[0], recv.at[n], {"tp": sibling}).wait_recv()

        for dk in reversed(range(1, n_kv)):
            send(block, send_a.at[dk], {"kv": flip(me_k, dk)})
        for dk in range(n_kv):
            here = me_y * n_kv + flip(me_k, dk)
            if dk:
                landed(ours, here, recv_ours)
            for dy in range(1, n_y):
                send(here, send_y.at[dy * n_kv + dk], {"tp": flip(me_t, 2 * dy)})
            send(here, send_b.at[dk], {"tp": sibling})
        for dy in range(1, n_y):
            for dk in range(n_kv):
                here = flip(me_y, dy) * n_kv + flip(me_k, dk)
                landed(ours, here, recv_ours)
                send(here, send_b.at[dy * n_kv + dk], {"tp": sibling})
        for dy in range(n_y):
            for dk in range(n_kv):
                landed(other, flip(me_y, dy) * n_kv + flip(me_k, dk), recv_other)
        for copy in big:
            copy.wait()
        for copy in sends:
            copy.wait_send()

    for c in range(2):
        pl.when(core == c)(functools.partial(role, c))


def attend_kernel(
    group, lengths_ref, accepted_ref, low_ref, fresh_ref, table_ref, wq_ref, held_in,
    out_hbm, part_ref, stats_ref, held_ref, q_main, q_turn, bias, turned_ref, write,
):
    heads, whole, _ = wq_ref.shape
    seqs, _, span = held_ref.shape
    rank = part_ref.shape[-1]
    turn_dim = whole - rank
    half = turn_dim // 2
    props = q_main.shape[1] // heads
    power = (NOPE_DIM + turn_dim) ** (-0.5) * 1.4426950408889634
    rows = low_ref.shape[0]
    offset = lax.axis_index("kv") * span

    low = low_ref[...]
    cosine = table_ref[:rows, :turn_dim]
    sine = table_ref[:rows, turn_dim : 2 * turn_dim]
    for h in range(heads):
        main = dot_nt(low, wq_ref[h, :rank, :])
        front, back = wq_ref[h, rank : rank + half, :], wq_ref[h, rank + half :, :]
        turn = dot_nt(low, jnp.concatenate([front, back], axis=0))
        swapped = dot_nt(low, jnp.concatenate([back, front], axis=0))
        turned = turn * cosine + swapped * sine
        lines = slice(h * props, (h + 1) * props)
        q_main[:, lines, :] = main.astype(jnp.bfloat16).reshape(seqs, props, rank)
        q_turn[:, lines, :] = turned.astype(jnp.bfloat16).reshape(seqs, props, turn_dim)

    def patch(s, carry):
        rel = lengths_ref[s] + accepted_ref[s] - offset
        lines = pl.ds(pl.multiple_of(s * props, props), props)
        past = iota((props, span), 1) < rel
        bias[s] = jnp.where(past, 0.0, score_after_mask * 1.5)
        first = lax.shift_right_arithmetic(rel, 7)
        last = lax.shift_right_arithmetic(rel + props - 1, 7)
        for more in range(2):
            chunk = first + more

            @pl.when((chunk >= 0) & (chunk < span // LANES) & (chunk <= last))
            def _():
                start = pl.multiple_of(chunk * LANES, LANES)
                slot = start - rel + iota((props, LANES), 1)
                onehot = (slot == iota((props, LANES), 0)).astype(jnp.float32).astype(jnp.bfloat16)
                reached = table_ref[lines, 2 * turn_dim : 2 * turn_dim + props]
                seen = (slot < 0) | (dot(reached.astype(jnp.bfloat16), onehot) > 0.5)
                bias[s, :, pl.ds(start, LANES)] = jnp.where(seen, 0.0, score_after_mask * 1.5)
                placed = lax.dot_general(
                    fresh_ref[lines, :whole], onehot, (((0,), (0,)), ((), ())),
                    preferred_element_type=jnp.float32,
                )
                slots = start - rel + iota(placed.shape, 1)
                old = held_ref[s, :, pl.ds(start, LANES)].astype(jnp.float32)
                new = jnp.where((slots >= 0) & (slots < props), placed, old)
                held_ref[s, :, pl.ds(start, LANES)] = new.astype(jnp.bfloat16)

        return carry

    lax.fori_loop(0, seqs, patch, 0)

    def write_out(s):
        return pltpu.make_async_copy(held_ref.at[s], out_hbm.at[s], write.at[s])

    for s in range(seqs):
        write_out(s).start()

    def step(i, carry):
        def score_of(s):
            scores = dot(q_main[s], held_ref[s, :rank, :]) + dot(q_turn[s], held_ref[s, rank:, :])
            return scores.reshape(heads, props, span) * power + bias[s][None]

        def finish(s, g, masked):
            top = jnp.max(masked, axis=-1, keepdims=True)
            weights = jnp.exp2(masked - jnp.maximum(top, -1e29))
            totals = jnp.sum(weights, axis=-1, keepdims=True)
            prob = weights.astype(jnp.bfloat16).reshape(heads * props, span)
            turned_ref[g] = held_ref[s, :rank, :].T
            weighted = dot(prob, turned_ref[g]).reshape(heads, props, rank)
            top = jnp.maximum(top * 0.6931471805599453, score_after_mask)
            part = (weighted / jnp.maximum(totals, 1.0)).astype(jnp.bfloat16)
            lane = iota((props, LANES), 1)
            stats = jnp.zeros((props, LANES), jnp.float32)
            lines = pl.ds(pl.multiple_of(s * props, props), props)
            for h in range(heads):
                part_ref[h, lines, :] = part[h]
                stats = jnp.where(lane == h, top[h], stats)
                stats = jnp.where(lane == heads + h, totals[h], stats)
            stats_ref[lines, :] = stats

        maskeds = [score_of(i * group + g) for g in range(group)]
        for g in range(group):
            finish(i * group + g, g, maskeds[g])
        return carry

    lax.fori_loop(0, seqs // group, step, 0)
    for s in range(seqs):
        write_out(s).wait()


def project_kernel(
    n_kv, n_tp,
    part_ref, stats_ref, wv_ref, w_out_ref, gain_ref, out_ref,
    vals, stat, got_vals, got_stat, attended, raw, got_raw, sums, result,
    send_v, recv_v, send_s, recv_s, send_a, recv_a, send_r, recv_r, send_q, recv_q, send_o, recv_o,
):
    me_k, me_t = lax.axis_index("kv"), lax.axis_index("tp")
    mine = me_t * n_kv + me_k
    heads, _, _ = part_ref.shape
    v_dim = wv_ref.shape[1]
    pieces, _, each, _ = vals.shape
    kv_peers = [flip(me_k, d) for d in range(n_kv)]
    tp_peers = [flip(me_t, d) for d in range(n_tp)]
    barrier = pltpu.get_barrier_semaphore()
    everyone = [(dk, dt) for dt in range(n_tp) for dk in range(n_kv) if dk or dt]
    for dk, dt in everyone:
        pl.semaphore_signal(
            barrier, inc=1,
            device_id={"kv": kv_peers[dk], "tp": tp_peers[dt]}, device_id_type=MESH,
        )
    sends = []

    line, lane = iota((8, LANES), 0), iota((8, LANES), 1)
    tops = (line < heads) & (lane == line)
    counts = (line >= 4) & (line < 4 + heads) & (lane == line - 4 + heads)
    pick = jnp.where(tops | counts, 1.0, 0.0)
    values = jnp.concatenate([dot_nt(part_ref[h], wv_ref[h]) for h in range(heads)], axis=1)
    for c in range(pieces):
        for j in range(n_kv):
            lines = slice((j * pieces + c) * each, (j * pieces + c + 1) * each)
            vals[c, j] = values[lines].astype(jnp.bfloat16)
            stat[c, j] = dot_nt(pick, stats_ref[lines, :], HIGHEST)
    pl.semaphore_wait(barrier, n_kv * n_tp - 1)

    def exchange(c, axis, peers, src_of, dst, own, send_sem, recv_sem):
        for d in reversed(range(1, len(peers))):
            copy = remote(
                src_of(peers[d]), dst.at[c, own], send_sem.at[c, d], recv_sem.at[c, own],
                {axis: peers[d]},
            )
            copy.start()
            sends.append(copy)

    def arrived(c, axis, peers, d, dst, send_sem, recv_sem):
        here = dst.at[c, peers[d]]
        remote(
            here, here, send_sem.at[c, d], recv_sem.at[c, peers[d]], {axis: peers[d]}
        ).wait_recv()

    for c in range(pieces):
        exchange(c, "kv", kv_peers, lambda p: stat.at[c, p], got_stat, me_k, send_s, recv_s)
        exchange(c, "kv", kv_peers, lambda p: vals.at[c, p], got_vals, me_k, send_v, recv_v)

    eye = iota((each, each), 0) == iota((each, each), 1)
    wide = iota((each, heads * v_dim), 1)
    for c in range(pieces):
        for d in range(1, n_kv):
            arrived(c, "kv", kv_peers, d, got_stat, send_s, recv_s)
        all_stats = [stat[c, me_k]] + [got_stat[c, p] for p in kv_peers[1:]]
        largest = all_stats[0]
        for one in all_stats[1:]:
            largest = jnp.maximum(largest, one)
        largest = largest[:4]
        shares = [one[4:] * jnp.exp(one[:4] - largest) for one in all_stats]
        shares = dot_nt(eye.astype(jnp.float32), jnp.concatenate(shares, axis=0), HIGHEST)
        summed = None
        for d in range(n_kv):
            share = shares[:, 4 * d : 4 * d + 1]
            for h in range(1, heads):
                share = jnp.where(wide >= h * v_dim, shares[:, 4 * d + h : 4 * d + h + 1], share)
            share = jnp.broadcast_to(share, wide.shape)
            if d:
                arrived(c, "kv", kv_peers, d, got_vals, send_v, recv_v)
            block = got_vals[c, kv_peers[d]] if d else vals[c, me_k]
            term = share * block.astype(jnp.float32)
            summed = term if summed is None else summed + term
            weight = share if d == 0 else weight + share
        attended[c, me_k] = (summed / weight).astype(jnp.bfloat16)
        exchange(
            c, "kv", kv_peers, lambda p: attended.at[c, me_k], attended, me_k, send_a, recv_a
        )

    share_rows, cols = raw.shape[2:]
    for c in range(pieces):
        for d in range(1, n_kv):
            arrived(c, "kv", kv_peers, d, attended, send_a, recv_a)
        lines = [attended[c, j].astype(jnp.float32) for j in range(n_kv)]
        lines = dot(jnp.concatenate(lines, axis=0).astype(jnp.bfloat16), w_out_ref[...])
        for t in range(n_tp):
            raw[c, t] = lines[t * share_rows : (t + 1) * share_rows].astype(jnp.bfloat16)
        exchange(c, "tp", tp_peers, lambda p: raw.at[c, p], got_raw, me_t, send_r, recv_r)

    for c in range(pieces):
        mixed = raw[c, me_t].astype(jnp.float32)
        for d in range(1, n_tp):
            arrived(c, "tp", tp_peers, d, got_raw, send_r, recv_r)
            mixed = mixed + got_raw[c, tp_peers[d]].astype(jnp.float32)
        result[c, me_t] = mixed.astype(jnp.bfloat16)
        sums[c, mine] = dot_nt(jnp.ones((8, cols), jnp.float32), mixed * mixed, HIGHEST)
        for n, (dk, dt) in reversed(list(enumerate(everyone))):
            copy = remote(
                sums.at[c, mine], sums.at[c, mine], send_q.at[c, n], recv_q.at[c, mine],
                {"kv": kv_peers[dk], "tp": tp_peers[dt]},
            )
            copy.start()
            sends.append(copy)
        exchange(c, "tp", tp_peers, lambda p: result.at[c, me_t], result, me_t, send_o, recv_o)

    eye = iota((share_rows, share_rows), 0) == iota((share_rows, share_rows), 1)
    for c in range(pieces):
        for d in range(1, n_tp):
            arrived(c, "tp", tp_peers, d, result, send_o, recv_o)
        for n, (dk, dt) in enumerate(everyone):
            source = tp_peers[dt] * n_kv + kv_peers[dk]
            here = sums.at[c, source]
            remote(
                here, here, send_q.at[c, n], recv_q.at[c, source],
                {"kv": kv_peers[dk], "tp": tp_peers[dt]},
            ).wait_recv()
        for t in range(n_tp):
            square = sums[c, t * n_kv]
            for j in range(1, n_kv):
                square = square + sums[c, t * n_kv + j]
            norm = lax.rsqrt(square / (cols * n_kv) + epsilon)
            column = jnp.sum(jnp.where(eye, norm[:1], 0.0), axis=1, keepdims=True)
            rows = result[c, t].astype(jnp.float32) * column * gain_ref[...]
            for o in range(share_rows // each):
                out_ref[t, o, c] = rows[o * each : (o + 1) * each].astype(jnp.bfloat16)
    for copy in sends:
        copy.wait_send()


def up(value, to):
    return -(-value // to) * to


def local(
    n_kv,
    n_tp,
    activations,
    latent_cache,
    lengths,
    accepted,
    parents,
    w_query_down,
    w_key_down,
    gain_input,
    gain_query,
    gain_key,
    w_query,
    w_value,
    w_out,
    gain_output,
):
    bf16, f32 = jnp.bfloat16, jnp.float32
    seqs, props = parents.shape
    rows, features = activations.shape
    heads = w_query.shape[1]
    q_rank, kv_rank = gain_query.shape[0], gain_key.shape[0]
    whole = latent_cache.shape[-1]
    turn_dim = whole - kv_rank
    half = turn_dim // 2
    span = latent_cache.shape[1]
    v_dim = w_value.shape[-1]
    cols = w_out.shape[1]
    n_dev = n_kv * n_tp
    me_t = lax.axis_index("tp")

    n_y = n_tp // 2
    blocks = n_y * n_kv
    few = rows // blocks
    each = up(few, 8)
    wide = up(whole, LANES)
    frequency = rope_base ** (-jnp.arange(half, dtype=f32) / half)
    dma = pltpu.SemaphoreType.DMA
    hbm = pl.BlockSpec(memory_space=pl.ANY)
    far = lambda array: pltpu.with_memory_space_constraint(array, pltpu.HBM)
    q_all, k_all, table, expand, held = pl.pallas_call(
        functools.partial(compress_kernel, n_kv, n_tp, few),
        name="compress",
        out_shape=(
            jax.ShapeDtypeStruct((blocks, each, q_rank), bf16),
            jax.ShapeDtypeStruct((blocks, each, wide), bf16),
            jax.ShapeDtypeStruct((rows + 8, LANES), f32),
            pltpu.VMEM((heads, whole, q_rank), bf16),
            pltpu.VMEM((seqs, whole, span), bf16),
        ),
        in_specs=[hbm] * 9 + [VMEM] + [hbm] * 2,
        out_specs=(VMEM,) * 5,
        scratch_shapes=[
            pltpu.VMEM((features, rows), bf16),
            pltpu.VMEM((features, q_rank), bf16),
            pltpu.VMEM((features, whole), bf16),
            pltpu.VMEM((features,), bf16),
            pltpu.VMEM((q_rank,), bf16),
            pltpu.VMEM((kv_rank,), bf16),
            pltpu.VMEM((props, seqs), jnp.int32),
            pltpu.SMEM((seqs,), jnp.int32),
            pltpu.SMEM((seqs,), jnp.int32),
            pltpu.VMEM((features, wide), bf16),
            pltpu.VMEM((n_y, n_kv * each // 2, 2 * features), bf16),
            pltpu.VMEM((n_tp, n_kv * each // 2, 2 * features), bf16),
            pltpu.VMEM((n_tp, features, q_rank), bf16),
            pltpu.VMEM((n_tp, features, wide), bf16),
            pltpu.VMEM((n_kv, each, q_rank), f32),
            pltpu.VMEM((n_kv, each, q_rank), f32),
            pltpu.VMEM((n_kv, each, wide), bf16),
            pltpu.VMEM((n_kv, each, wide), bf16),
            pltpu.VMEM((n_tp, 8, LANES), f32),
            pltpu.VMEM((n_kv, 8, LANES), f32),
            dma((10,)), dma((seqs,)),
            dma((n_tp,)), dma((n_tp,)), dma((n_tp,)), dma((n_tp,)),
            dma((n_tp,)), dma((n_tp,)), dma((n_kv,)), dma((n_kv,)), dma((n_kv,)), dma((n_kv,)),
            dma((n_kv,)), dma((blocks,)), dma((blocks,)), dma((blocks,)), dma((blocks,)),
        ],
        compiler_params=pltpu.CompilerParams(
            collective_id=0, has_side_effects=True, vmem_limit_bytes=20 * 1024 * 1024
        ),
    )(
        far(activations.T), far(w_query_down), far(w_key_down),
        far(gain_input), far(gain_query), far(gain_key), far(parents.T),
        far(lengths), far(accepted), frequency[:, None],
        far(w_query.transpose(1, 2, 0)), far(latent_cache.transpose(0, 2, 1)),
    )
    query_low = q_all[:, :few].reshape(rows, q_rank)
    fresh = k_all[:, :few].reshape(rows, wide)

    group = next(g for g in (3, 2, 1) if seqs % g == 0)
    smem = pl.BlockSpec(memory_space=pltpu.SMEM)
    updated, part, stats, _ = pl.pallas_call(
        functools.partial(attend_kernel, group),
        name="attend",
        out_shape=(
            jax.ShapeDtypeStruct((seqs, whole, span), bf16),
            jax.ShapeDtypeStruct((heads, rows, kv_rank), bf16),
            jax.ShapeDtypeStruct((rows, LANES), f32),
            pltpu.VMEM((seqs, whole, span), bf16),
        ),
        in_specs=[smem] * 2 + [VMEM] * 5,
        out_specs=(hbm, VMEM, VMEM, VMEM),
        scratch_shapes=[
            pltpu.VMEM((seqs, heads * props, kv_rank), bf16),
            pltpu.VMEM((seqs, heads * props, turn_dim), bf16),
            pltpu.VMEM((seqs, props, span), f32),
            pltpu.VMEM((group, span, kv_rank), bf16),
            dma((seqs,)),
        ],
        input_output_aliases={6: 3},
        compiler_params=pltpu.CompilerParams(vmem_limit_bytes=24 * 1024 * 1024),
    )(
        lengths, accepted, query_low, fresh, table,
        pltpu.with_memory_space_constraint(expand, pltpu.VMEM),
        pltpu.with_memory_space_constraint(held, pltpu.VMEM),
    )

    wv = lax.dynamic_slice_in_dim(w_value.transpose(0, 2, 1), me_t * heads, heads, 0)
    per_kv, share = rows // n_kv, n_kv // n_tp
    pieces = 1
    lot = per_kv // pieces
    mixed = pl.pallas_call(
        functools.partial(project_kernel, n_kv, n_tp),
        name="project",
        out_shape=jax.ShapeDtypeStruct((n_tp, share, pieces, lot, cols), bf16),
        in_specs=[VMEM] * 5,
        out_specs=VMEM,
        scratch_shapes=[
            pltpu.VMEM((pieces, n_kv, lot, heads * v_dim), bf16),
            pltpu.VMEM((pieces, n_kv, 8, lot), f32),
            pltpu.VMEM((pieces, n_kv, lot, heads * v_dim), bf16),
            pltpu.VMEM((pieces, n_kv, 8, lot), f32),
            pltpu.VMEM((pieces, n_kv, lot, heads * v_dim), bf16),
            pltpu.VMEM((pieces, n_tp, share * lot, cols), bf16),
            pltpu.VMEM((pieces, n_tp, share * lot, cols), bf16),
            pltpu.VMEM((pieces, n_dev, 8, share * lot), f32),
            pltpu.VMEM((pieces, n_tp, share * lot, cols), bf16),
        ]
        + [dma((pieces, n)) for n in (n_kv,) * 6 + (n_tp,) * 2 + (n_dev,) * 2 + (n_tp,) * 2],
        compiler_params=pltpu.CompilerParams(
            collective_id=1, has_side_effects=True, vmem_limit_bytes=32 * 1024 * 1024
        ),
    )(part, stats, wv, w_out, gain_output.astype(f32)[None])
    return (mixed.reshape(rows, cols), updated.transpose(0, 2, 1))


def solution(mesh):
    in_specs = (
        P(None, ("kv", "tp")),
        P(None, "kv", None),
        P(),
        P(),
        P(),
        P(("kv", "tp"), None),
        P(("kv", "tp"), None),
        P(("kv", "tp")),
        P(),
        P(),
        P(None, "tp", None),
        P(),
        P("tp", "kv"),
        P("kv"),
    )
    out_specs = (P(None, "kv"), P(None, "kv", None))
    body = functools.partial(local, mesh.shape["kv"], mesh.shape["tp"])
    return jax.shard_map(body, mesh=mesh, in_specs=in_specs, out_specs=out_specs, check_vma=False)
```
